32 devices in a mesh: sp: 8 (over z, y), tp: 4 (over x, core).
Axes of the slice: x: 2, y: 2, z: 4, core: 2. Of those that a mesh axis runs over, the one named last changes fastest.
Arguments:
- stream: bfloat16 [16384, 4096], P('sp', 'tp'), may hold values from -18 to 18
- doc_ids: int32 [16384], P('sp'), may hold values from 0 to 1, never falling along the last dimension, each value on 1 to 12288 neighbouring positions
- norm_gain: bfloat16 [3, 4096], replicated, may hold values from 0.099609375 to 1.8984375
- proj_in: bfloat16 [3, 4096, 1024], P(None, 'tp', 'sp'), may hold values from -0.09375 to 0.09375
- mix_pool: bfloat16 [3, 8, 128, 128], replicated, may hold values from -0.5 to 0.5
- pool_gain: bfloat16 [3, 1024], replicated, may hold values from 0.099609375 to 1.8984375
- proj_out: bfloat16 [3, 1024, 4096], P(None, 'sp', 'tp'), may hold values from -0.1875 to 0.1875
Outputs:
- stream_out: bfloat16 [16384, 4096], P('sp', 'tp')
The draws below stay inside these ranges and needn't reach their ends.
Inputs may be any that keep to these rules, and one draw needn't show every extreme that they name: `doc_ids`: document numbers never fall along the sequence; each document holds 1 to 12288 positions, one exactly that many.
All inputs are finite; a program needn't handle non-finite values.
Results may differ from the reference program's by a relative error of at most 0.02.
Values may be sent and summed in bfloat16 or wider, within the bound.
A program may use at most 64 MiB of HBM per device.

```python
import math
import jax
import jax.numpy as jnp
import numpy as np
from jax import lax

D = 4096
POOL = 1024
GROUP = 128
LAYERS = 3
TOK = 2048
GROUPS = 8
TOKENS = 16384
DOCS = 2
N_TP = 4


def draw_stream(key, part):
    key_base = jax.random.fold_in(key, 11)
    key_cols = jax.random.fold_in(key, 12)
    column_scale = jnp.exp(jax.random.uniform(key_cols, (32,), jnp.float32, -1.1, 1.1))
    column_scale = jnp.repeat(column_scale, D // 32)
    base = jnp.clip(jax.random.normal(key_base, (TOKENS, D), jnp.float32), -6.0, 6.0)
    values = jnp.clip(base * column_scale[None, :], -18.0, 18.0)
    return values.astype(jnp.bfloat16)


def block_scale(own_key, shape, pieces, low, high):
    level, own = 1.0, jax.random.fold_in(own_key, 6)
    for position, blocks in pieces:
        steps = jnp.exp(jax.random.uniform(jax.random.fold_in(own, position), (blocks,), jnp.float32, low / len(pieces), high / len(pieces)))
        level = level * jnp.repeat(steps, shape[position] // blocks).reshape([-1 if axis == position else 1 for axis in range(len(shape))])
    return level


def split_up(count, total, limit, lean):
    portions = [(1 << 20) // math.isqrt(rank ** lean) + 1 for rank in range(2, count + 1)]
    spare, given = total - limit - (count - 1), [1] * (count - 1)
    while spare > 0:
        movable = [i for i in range(count - 1) if given[i] < limit]
        whole, left = sum([portions[i] for i in movable]), spare
        for i in movable:
            more = min(limit - given[i], max(1, left * portions[i] // whole), spare)
            given[i] = given[i] + more
            spare = spare - more
    return np.array([limit] + given)


def ragged(rng, count, total, limit, slope):
    if count == 2:
        one = jax.random.randint(rng, (), max(1, total - limit), min(limit, total - 1) + 1)
        return jnp.stack([one, total - one])
    lengths = jnp.asarray(split_up(count, total, limit, slope), jnp.int32)
    twos = (count - 1) // 2
    source_of, receiver = lengths[1:1 + 2 * twos:2], lengths[2:2 + 2 * twos:2]
    room = jnp.minimum(source_of - 1, limit - receiver)
    passed = jax.random.randint(jax.random.fold_in(rng, 1), (twos,), 0, 1 << 20) % (room + 1)
    lengths = lengths.at[1:1 + 2 * twos:2].set(source_of - passed).at[2:2 + 2 * twos:2].set(receiver + passed)
    return lengths[jax.random.permutation(jax.random.fold_in(rng, 2), count)]


def normal_values(rng, dims, deviation, bound, shards=(), held_as=jnp.bfloat16):
    entries = jax.random.normal(rng, dims, jnp.float32) * deviation
    if len(shards) > 0:
        entries = block_scale(rng, dims, shards, -0.22, 0.18) * entries
    return jnp.clip(entries, min=-bound, max=bound).astype(held_as)


def setup_inputs(seed: int = 0) -> dict:
    key_of = jax.random.split(jax.random.key(seed), 8)
    return {
        "stream": draw_stream(jax.random.fold_in(key_of[7], 71), 0),
        "doc_ids": jnp.searchsorted(jnp.cumsum(ragged(key_of[1], DOCS, TOKENS, 6 * TOK, 1)), jnp.arange(TOKENS), side="right").astype(jnp.int32),
        "norm_gain": jnp.clip(1.0 + 0.18 * jax.random.normal(key_of[2], (LAYERS, D), jnp.float32), 0.099609375, 1.8984375).astype(jnp.bfloat16),
        "proj_in": normal_values(key_of[3], (LAYERS, D, POOL), D ** -0.5, 0.09375, ((1, 4), (2, 8))),
        "mix_pool": normal_values(key_of[4], (LAYERS, GROUPS, GROUP, GROUP), GROUP ** -0.5, 0.5),
        "pool_gain": jnp.clip(1.0 + 0.18 * jax.random.normal(key_of[5], (LAYERS, POOL), jnp.float32), 0.099609375, 1.8984375).astype(jnp.bfloat16),
        "proj_out": normal_values(key_of[6], (LAYERS, POOL, D), POOL ** -0.5, 0.1875, ((1, 8), (2, 4))),
    }


epsilon = 1e-06
span_reach = 15

def span_pool(padded, labels, widths):
    kept = padded.shape[0] - span_reach
    own_label = labels[span_reach:]
    summed = jnp.zeros((kept, padded.shape[1]), jnp.float32)
    counted = jnp.zeros((kept, padded.shape[1]), jnp.float32)
    for offset in range(span_reach + 1):
        first = span_reach - offset
        member = (labels[first:first + kept] == own_label)[:, None] & (offset < widths)[None, :]
        factor = member.astype(jnp.float32)
        summed = summed + padded[first:first + kept] * factor
        counted = counted + factor
    return summed / counted - padded[span_reach:]

def reference(stream, doc_ids, norm_gain, proj_in, mix_pool, pool_gain, proj_out):
    hidden = stream
    labels = (doc_ids + 1).astype(jnp.int32)
    tags = jnp.concatenate([jnp.zeros((span_reach,), jnp.int32), labels])
    channel = jnp.arange(POOL, dtype=jnp.int32)
    widths = jnp.left_shift(jnp.int32(2), channel // GROUP % 4)
    block = D // N_TP
    for layer in range(LAYERS):
        wide = hidden.astype(jnp.float32)
        scale_rows = lax.rsqrt(lax.optimization_barrier(jnp.mean(wide * wide, axis=1)) + epsilon)
        gained = (wide * norm_gain[layer].astype(jnp.float32)[None, :]).astype(jnp.bfloat16)
        summed_in = jnp.zeros((hidden.shape[0], POOL), jnp.float32)
        for piece in range(N_TP):
            partial_value = jnp.dot(gained[:, piece * block:(piece + 1) * block], proj_in[layer, piece * block:(piece + 1) * block], preferred_element_type=jnp.float32)
            summed_in = summed_in + lax.optimization_barrier(partial_value.astype(jnp.bfloat16)).astype(jnp.float32)
        mixed_in = (summed_in * scale_rows[:, None]).astype(jnp.bfloat16)
        padded = jnp.concatenate([jnp.zeros((span_reach, POOL), jnp.float32), mixed_in.astype(jnp.float32)])
        pooled = span_pool(padded, tags, widths).astype(jnp.bfloat16)
        grouped = pooled.reshape(hidden.shape[0], GROUPS, GROUP).astype(jnp.float32)
        blended = jnp.einsum('tgc,gcd->tgd', grouped, mix_pool[layer].astype(jnp.float32)).reshape(hidden.shape[0], POOL)
        mixed = (blended * pool_gain[layer].astype(jnp.float32)[None, :]).astype(jnp.bfloat16)
        update = jnp.dot(mixed, proj_out[layer], preferred_element_type=jnp.float32)
        hidden = (wide + update).astype(jnp.bfloat16)
    return hidden
```

```python
import functools

import jax
import jax.numpy as jnp
from jax import lax
from jax.experimental import pallas as pl
from jax.experimental.pallas import tpu as pltpu
from jax.sharding import PartitionSpec as P

EPSILON = 1e-06
HALO = 16
CHUNKS = 8
EDGE = 3
RING = 8
LAYERS = 3
MESH = pl.DeviceIdType.MESH
F32, BF16 = jnp.float32, jnp.bfloat16


def mixer(sp, tp, x_hbm, doc_ref, gains_ref, win_hbm, mix_ref, pgains_ref, wout_hbm, o_hbm,
          h, win, wout, gbuf, send1, own1, recv1, sum2, recv2, mixed, zbuf, hrecv,
          sq_own, sq_in, scale_ref, labels, before_labels, pos_ref, gain_ref, pgain_ref,
          xs, ws, os, ls, lr, ring_s, ring_r, sqs, sqr, s1, r1, s2, r2, s3, r3, hs, hr):
    layers, model_dev, chan_dev = win_hbm.shape
    tokens = h.shape[0]
    rows = tokens // CHUNKS
    channels = chan_dev * sp
    half = channels // 2
    group = mix_ref.shape[-1]
    own_groups = half // group
    model = model_dev * tp
    row_dev = wout_hbm.shape[1]
    last = CHUNKS - 1
    s, t = lax.axis_index("sp"), lax.axis_index("tp")
    core = lax.rem(t, 2)
    partner = t + 1 - 2 * core
    across = lax.rem(t + 2, tp)
    diagonal = lax.rem(partner + 2, tp)

    def place(device):
        z, y = device // 2, lax.rem(device, 2)
        return z * (1 - y) + (sp - 1 - z) * y

    def device_at(place):
        up = place // (sp // 2)
        return 2 * (place * (1 - up) + (sp - 1 - place) * up) + up

    here = place(s)
    after, before = device_at(lax.rem(here + 1, sp)), device_at(lax.rem(here + sp - 1, sp))
    following, leading = lax.rem(s + 1, sp), lax.rem(s + sp - 1, sp)

    def columns(device):
        return pl.ds(pl.multiple_of(device * chan_dev, chan_dev), chan_dev)

    def ring_view(layer, side, piece, source):
        if side == 0:
            part = model_dev // 2
            return win.at[layer, pl.ds(pl.multiple_of(piece * part, part), part), columns(source)]
        part = row_dev // 2
        return wout.at[layer, pl.ds(pl.multiple_of(source * row_dev + piece * part, part), part)]

    def ring_copy(layer, side, way, turn, back):
        hop = turn // 2 + back
        piece = lax.rem(turn + way, 2)
        origin = here - hop + sp if way == 0 else here + hop
        view = ring_view(layer, side, piece, device_at(lax.rem(origin, sp)))
        return pltpu.make_async_remote_copy(
            src_ref=view, dst_ref=view,
            send_sem=ring_s.at[layer, side, way, turn], recv_sem=ring_r.at[layer, side, way, turn],
            device_id={"sp": after if way == 0 else before}, device_id_type=MESH)

    turns = sp - 1
    items = 2 * layers

    def arrive(index):
        item, turn = index // turns, lax.rem(index, turns)
        layer, side = item // 2, lax.rem(item, 2)
        for which in range(2):
            @pl.when(side == which)
            def _():
                for way in range(2):
                    ring_copy(layer, which, way, turn, 1).wait_recv()

                @pl.when(turn < turns - 2)
                def _():
                    for way in range(2):
                        ring_copy(layer, which, way, turn + 2, 0).start()

                @pl.when((turn >= turns - 3) & (turn < turns - 1) & (item + 1 < items))
                def _():
                    for way in range(2):
                        ring_copy(layer + which, 1 - which, way, turn - (turns - 3), 0).start()

    def at(i):
        return pl.ds(pl.multiple_of(i * rows, rows), rows)

    def load_x(i):
        return pltpu.make_async_copy(x_hbm.at[at(i)], h.at[at(i)], xs.at[i])

    def load_w(layer, side):
        if side == 0:
            return pltpu.make_async_copy(win_hbm.at[layer], win.at[layer, :, columns(s)], ws.at[layer, side])
        return pltpu.make_async_copy(
            wout_hbm.at[layer], wout.at[layer, pl.ds(pl.multiple_of(s * row_dev, row_dev), row_dev)], ws.at[layer, side])

    def store_out(i):
        return pltpu.make_async_copy(h.at[at(i)], o_hbm.at[at(i)], os.at[i])

    load_w(0, 0).start()
    for i in range(CHUNKS):
        load_x(last - i).start()
    for layer in range(layers):
        for side in range(2):
            if layer + side > 0:
                load_w(layer, side).start()

    barrier = pltpu.get_barrier_semaphore()
    peers = ({"tp": partner}, {"tp": across}, {"tp": diagonal},
             {"sp": after}, {"sp": before}, {"sp": following}, {"sp": leading})
    for peer in peers:
        pl.semaphore_signal(barrier, inc=1, device_id=peer, device_id_type=MESH)
    own_gain = gains_ref[:, pl.ds(pl.multiple_of(t * model_dev, model_dev), model_dev)].astype(F32)
    own_pgain = pgains_ref[:, pl.ds(pl.multiple_of(core * half, half), half)].astype(F32)
    for layer in range(layers):
        gain_ref[layer] = own_gain[layer:layer + 1]
        pgain_ref[layer] = own_pgain[layer:layer + 1]
    reach = 2 * HALO
    documents = doc_ref[...].astype(F32)
    for j in range(tokens // 128):
        labels[pl.ds(reach + j * 128, 128)] = jnp.broadcast_to(documents[j:j + 1], (128, 128)).T
    load_w(0, 0).wait()
    pl.semaphore_wait(barrier, len(peers))
    for turn in range(2):
        for way in range(2):
            ring_copy(0, 0, way, turn, 0).start()
    label_copy = pltpu.make_async_remote_copy(
        src_ref=labels.at[pl.ds(tokens, reach)], dst_ref=before_labels, send_sem=ls, recv_sem=lr,
        device_id={"sp": following}, device_id_type=MESH)
    label_copy.start()
    for i in range(CHUNKS):
        load_x(last - i).wait()
    for layer in range(layers):
        for side in range(2):
            if layer + side > 0:
                load_w(layer, side).wait()

    def distances(ext):
        run = (pltpu.roll(ext, 1, 0) == ext).astype(F32)
        size = 1
        while size < HALO:
            run = run + jnp.where(run == float(size), pltpu.roll(run, size, 0), 0.0)
            size *= 2
        return run[HALO:]

    def prepare():
        label_copy.wait()
        labels[pl.ds(0, reach)] = jnp.where(s == 0, -1.0, before_labels[...])
        pos_ref[pl.ds(0, HALO)] = distances(labels[pl.ds(0, reach)])

        @pl.loop(0, CHUNKS)
        def _(i):
            pos_ref[pl.ds(pl.multiple_of(HALO + i * rows, HALO), rows)] = distances(
                labels[pl.ds(pl.multiple_of(HALO + i * rows, HALO), rows + HALO)])

    def copy_sq(layer, i):
        par = lax.rem(layer, 2)
        return [pltpu.make_async_remote_copy(
            src_ref=sq_own.at[i], dst_ref=sq_in.at[j, par, i], send_sem=sqs.at[j, i], recv_sem=sqr.at[j, par, i],
            device_id={"tp": peer}, device_id_type=MESH)
            for j, peer in enumerate((partner, across, diagonal))]

    def copy1(i, lg):
        return pltpu.make_async_remote_copy(
            src_ref=send1.at[lg, i], dst_ref=recv1.at[lg, i], send_sem=s1.at[lg, i], recv_sem=r1.at[lg, i],
            device_id={"tp": partner}, device_id_type=MESH)

    def copy2(layer, i, lg):
        par = lax.rem(layer, 2)
        return pltpu.make_async_remote_copy(
            src_ref=sum2.at[lg, i], dst_ref=recv2.at[par, lg, i], send_sem=s2.at[lg, i], recv_sem=r2.at[par, lg, i],
            device_id={"tp": across}, device_id_type=MESH)

    def copy3(i, side, lg):
        view = mixed.at[i, :, pl.ds(pl.multiple_of(side * half + lg * group, group), group)]
        return pltpu.make_async_remote_copy(
            src_ref=view, dst_ref=view, send_sem=s3.at[lg, i], recv_sem=r3.at[lg, i],
            device_id={"tp": partner}, device_id_type=MESH)

    def halo_copy(layer, lg):
        return pltpu.make_async_remote_copy(
            src_ref=zbuf.at[lg, pl.ds(tokens, HALO)], dst_ref=hrecv.at[layer, lg],
            send_sem=hs.at[layer, lg], recv_sem=hr.at[layer, lg],
            device_id={"sp": following}, device_id_type=MESH)

    def groups_of(distance):
        return (device_at(lax.rem(here - distance + sp, sp)), device_at(lax.rem(here + distance, sp)))

    def owned(g):
        return g // own_groups == core

    def local(g):
        return lax.rem(g, own_groups)

    def gained_of(layer, i):
        wide = h[at(i)].astype(F32)
        squares = wide * wide
        lanes = squares[:, :128]
        for j in range(1, model_dev // 128):
            lanes = lanes + squares[:, j * 128:(j + 1) * 128]
        sq_own[i] = jnp.sum(lanes.T, axis=0, keepdims=True)
        gained = (wide * gain_ref[layer]).astype(BF16)
        for c in copy_sq(layer, i):
            c.start()
        return gained

    def deliver(i, g, value):
        @pl.when(owned(g))
        def _():
            own1[local(g), i] = value

        @pl.when(jnp.logical_not(owned(g)))
        def _():
            send1[local(g), i] = value
            copy1(i, local(g)).start()

    def project_groups(layer, distance, i):
        low, high = groups_of(distance)

        @pl.when(lax.rem(distance, sp // 2) == 0)
        def _():
            part = jnp.dot(gbuf[i], win[layer, :, columns(low)], preferred_element_type=F32).astype(BF16)
            deliver(i, low, part)

        @pl.when(lax.rem(distance, sp // 2) > 0)
        def _():
            weights = jnp.concatenate([win[layer, :, columns(low)], win[layer, :, columns(high)]], axis=1)
            part = jnp.dot(gbuf[i], weights, preferred_element_type=F32).astype(BF16)
            deliver(i, low, part[:, :group])
            deliver(i, high, part[:, group:])

    def project(layer, i):
        gained = gained_of(layer, i)
        other = pl.ds(pl.multiple_of((1 - core) * half, half), half)
        part = jnp.dot(gained, win[layer, :, other], preferred_element_type=F32).astype(BF16)
        for lg in range(own_groups):
            send1[lg, i] = part[:, lg * group:(lg + 1) * group]
            copy1(i, lg).start()
        mine = pl.ds(pl.multiple_of(core * half, half), half)
        part = jnp.dot(gained, win[layer, :, mine], preferred_element_type=F32).astype(BF16)
        for lg in range(own_groups):
            own1[lg, i] = part[:, lg * group:(lg + 1) * group]

    def add_up(layer, i, lg):
        sum2[lg, i] = (own1[lg, i].astype(F32) + recv1[lg, i].astype(F32)).astype(BF16)
        copy2(layer, i, lg).start()

    def each_group(distance, act):
        low, high = groups_of(distance)
        act(low)

        @pl.when(lax.rem(distance, sp // 2) > 0)
        def _():
            act(high)

    def join_groups(layer, distance, i):
        def act(g):
            @pl.when(owned(g))
            def _():
                copy1(i, local(g)).wait_recv()
                add_up(layer, i, local(g))

            @pl.when(jnp.logical_not(owned(g)))
            def _():
                copy1(i, local(g)).wait_send()
        each_group(distance, act)

    def join(layer, i):
        for lg in range(own_groups):
            copy1(i, lg).wait()
            add_up(layer, i, lg)

    def rescale(layer, i):
        par = lax.rem(layer, 2)
        total = sq_own[i]
        for j, c in enumerate(copy_sq(layer, i)):
            c.wait()
            total = total + sq_in[j, par, i]
        scale_ref[i] = jnp.broadcast_to(lax.rsqrt(total / model + EPSILON), (128, rows)).T

    def normalise(layer, i, lg):
        par = lax.rem(layer, 2)
        copy2(layer, i, lg).wait()
        summed = sum2[lg, i].astype(F32) + recv2[par, lg, i].astype(F32)
        zbuf[lg, pl.ds(pl.multiple_of(HALO + i * rows, HALO), rows)] = (summed * scale_ref[i]).astype(BF16)

        @pl.when(i == last)
        def _():
            halo_copy(layer, lg).start()

    def pool(layer, i, lg):
        @pl.when(i == 0)
        def _():
            halo_copy(layer, lg).wait()
            zbuf[lg, pl.ds(0, HALO)] = hrecv[layer, lg]

        wide_at = pl.ds(pl.multiple_of(i * rows, HALO), rows + HALO)
        pos = pos_ref[wide_at]
        z = zbuf[lg, wide_at].astype(F32)
        window = 2 ** (1 + lg % 4)
        total = z
        size = 1
        while size < window:
            total = total + jnp.where(pos >= size, pltpu.roll(total, size, 0), 0.0)
            size *= 2
        count = jnp.minimum(pos[HALO:] + 1.0, float(window))
        pooled = (total[HALO:] / count - z[HALO:]).astype(BF16)
        blended = jnp.dot(pooled, mix_ref[layer, core * own_groups + lg], preferred_element_type=F32)
        place_at = pl.ds(pl.multiple_of(core * half + lg * group, group), group)
        mixed[i, :, place_at] = (blended * pgain_ref[layer, :, lg * group:(lg + 1) * group]).astype(BF16)
        copy3(i, core, lg).start()

    def finish(layer, i):
        for lg in range(own_groups):
            copy3(i, core, lg).wait_send()
            copy3(i, 1 - core, lg).wait_recv()
        for j in range(2):
            cols = slice(j * (model_dev // 2), (j + 1) * (model_dev // 2))
            update = jnp.dot(mixed[i], wout[layer, :, cols], preferred_element_type=F32)
            h[at(i), cols] = (h[at(i), cols].astype(F32) + update).astype(BF16)

        @pl.when(layer == layers - 1)
        def _():
            store_out(i).start()

    spans = sp // 2 + 1

    @pl.loop(0, layers + 1)
    def _(layer):
        edge = EDGE + layer
        ending = layer // layers
        live = layer < layers
        slots = (spans + edge) * (1 - ending) + 2 * ending
        done = layer - 1

        @pl.loop(0, slots)
        def _(q):
            turn = 2 * (q - 1 + (sp - 1) * layer + 2 * (layer // 2))
            pumping = live & (turn < turns * items) & ((q > 0) | (layer > 1))
            early = (q > 0) & (q < spans - 1)

            @pl.when(pumping)
            def _():
                arrive(turn)

            @pl.when(pumping & early)
            def _():
                arrive(turn + 1)

            @pl.when(live & (q == 0))
            def _():
                @pl.loop(0, CHUNKS - edge)
                def _(j):
                    gbuf[last - j] = gained_of(layer, last - j)

            @pl.when(live & (q < spans))
            def _():
                @pl.loop(0, CHUNKS - edge)
                def _(j):
                    project_groups(layer, q, last - j)

            @pl.when(q >= spans)
            def _():
                project(layer, edge - 1 - (q - spans))

            @pl.when((layer == 0) & (q == 1))
            def _():
                prepare()

            @pl.when(live & (q > 1) & (q < spans + 2))
            def _():
                distance = q - 2

                @pl.loop(0, CHUNKS - edge)
                def _(j):
                    @pl.when(distance == 0)
                    def _():
                        rescale(layer, last - j)

                    def act(g):
                        @pl.when(owned(g))
                        def _():
                            normalise(layer, last - j, local(g))
                    each_group(distance, act)

                @pl.loop(0, CHUNKS - edge - 1)
                def _(j):
                    def act(g):
                        for lg in range(own_groups):
                            @pl.when(owned(g) & (local(g) == lg))
                            def _():
                                pool(layer, last - j, lg)
                    each_group(distance, act)

            old = (q < 2) & (layer > 0)

            @pl.when(old | (q >= spans + 2))
            def _():
                fresh = q // (spans + 2)
                of = layer - 1 + fresh
                i = (1 - q) * (1 - fresh) + (edge - 1 - (q - 2 - spans)) * fresh
                rescale(of, i)
                for lg in range(own_groups):
                    normalise(of, i, lg)

                @pl.loop(0, 1 + (1 - fresh) * q)
                def _(j):
                    for lg in range(own_groups):
                        pool(of, i + 1 - j, lg)

            @pl.when(pumping & jnp.logical_not(early))
            def _():
                arrive(turn + 1)

            @pl.when(live & (q < spans))
            def _():
                @pl.loop(0, CHUNKS - edge)
                def _(j):
                    join_groups(layer, q, last - j)

            @pl.when(q >= spans)
            def _():
                join(layer, edge - 1 - (q - spans))

            @pl.when((q == spans + 2) & live)
            def _():
                @pl.loop(0, CHUNKS - edge - 1)
                def _(j):
                    finish(layer, last - j)

            one = (q < 4) & (layer > 0)

            @pl.when(one | (q > spans + 2))
            def _():
                fresh = q // (spans + 3)
                first = (3 - q - q * ending) * (1 - fresh) + (edge - (q - spans - 3)) * fresh

                @pl.loop(0, 1 + ending)
                def _(j):
                    finish(layer - 1 + fresh, first - j)

    @pl.loop(0, layers)
    def _(layer):
        for side in range(2):
            for way in range(2):
                @pl.loop(0, turns)
                def _(turn):
                    ring_copy(layer, side, way, turn, 0).wait_send()

    @pl.loop(0, CHUNKS)
    def _(i):
        store_out(i).wait()


def body(sp, tp, stream, doc_ids, norm_gain, proj_in, mix_pool, pool_gain, proj_out):
    layers, model_dev, chan_dev = proj_in.shape
    tokens = stream.shape[0]
    rows = tokens // CHUNKS
    channels = chan_dev * sp
    half = channels // 2
    group = mix_pool.shape[-1]
    own = half // group
    dma, vmem = pltpu.SemaphoreType.DMA, pltpu.VMEM
    local, remote = pl.BlockSpec(memory_space=pltpu.VMEM), pl.BlockSpec(memory_space=pl.ANY)
    return pl.pallas_call(
        functools.partial(mixer, sp, tp),
        out_shape=jax.ShapeDtypeStruct(stream.shape, BF16),
        in_specs=[remote, local, local, remote, local, local, remote],
        out_specs=remote,
        scratch_shapes=[
            vmem((tokens, model_dev), BF16),
            vmem((layers, model_dev, channels), BF16),
            vmem((layers, channels, model_dev), BF16),
            vmem((CHUNKS, rows, model_dev), BF16),
            vmem((own, CHUNKS, rows, group), BF16),
            vmem((own, CHUNKS, rows, group), BF16),
            vmem((own, CHUNKS, rows, group), BF16),
            vmem((own, CHUNKS, rows, group), BF16),
            vmem((2, own, CHUNKS, rows, group), BF16),
            vmem((CHUNKS, rows, channels), BF16),
            vmem((own, HALO + tokens, group), BF16),
            vmem((layers, own, HALO, group), BF16),
            vmem((CHUNKS, 1, rows), F32),
            vmem((3, 2, CHUNKS, 1, rows), F32),
            vmem((CHUNKS, rows, 128), F32),
            vmem((2 * HALO + tokens, 128), F32),
            vmem((2 * HALO, 128), F32),
            vmem((HALO + tokens, 128), F32),
            vmem((layers, 1, model_dev), F32),
            vmem((layers, 1, half), F32),
            dma((CHUNKS,)), dma((layers, 2)), dma((CHUNKS,)),
            dma, dma,
            dma((layers, 2, 2, sp - 1)), dma((layers, 2, 2, sp - 1)),
            dma((3, CHUNKS)), dma((3, 2, CHUNKS)),
            dma((own, CHUNKS)), dma((own, CHUNKS)),
            dma((own, CHUNKS)), dma((2, own, CHUNKS)),
            dma((own, CHUNKS)), dma((own, CHUNKS)),
            dma((layers, own)), dma((layers, own)),
        ],
        compiler_params=pltpu.CompilerParams(
            collective_id=0, has_side_effects=True, vmem_limit_bytes=60 * 2**20),
    )(stream, doc_ids.reshape(-1, 128), norm_gain, proj_in, mix_pool, pool_gain, proj_out)


span_reach = 15


def shifted(value, axis, steps):
    count = lax.axis_size(axis)
    initial, last = (max(0, -steps), min(count, count - steps))
    return lax.ppermute(value, axis, [(source, source + steps) for source in range(initial, last)])


def span_pool(padded, labels, widths):
    kept = padded.shape[0] - span_reach
    own_label = labels[span_reach:]
    summed = jnp.zeros((kept, padded.shape[1]), jnp.float32)
    counted = jnp.zeros((kept, padded.shape[1]), jnp.float32)
    for offset in range(span_reach + 1):
        first = span_reach - offset
        member = (labels[first : first + kept] == own_label)[:, None] & (offset < widths)[None, :]
        factor = member.astype(jnp.float32)
        summed = summed + padded[first : first + kept] * factor
        counted = counted + factor
    return summed / counted - padded[span_reach:]


def plain_body(stream, doc_ids, norm_gain, proj_in, mix_pool, pool_gain, proj_out):
    width_dev = stream.shape[1]
    tp_count = lax.axis_size("tp")
    model_width = width_dev * tp_count
    group_size = mix_pool.shape[2]
    channels = proj_in.shape[2] * lax.axis_size("sp")
    local = channels // tp_count
    groups_dev = local // group_size
    column = lax.axis_index("tp")
    chan_ids = column * local + jnp.arange(local, dtype=jnp.int32)
    widths = jnp.left_shift(jnp.int32(2), chan_ids // group_size % 4)
    labels = (doc_ids + 1).astype(jnp.bfloat16)
    hidden_state = stream
    layer_count = proj_in.shape[0]
    in_whole, out_whole = (
        lax.all_gather(proj_in, "sp", axis=2, tiled=True),
        lax.all_gather(proj_out, "sp", axis=1, tiled=True),
    )
    for layer in range(layer_count):
        row_count = hidden_state.shape[0]
        wide = hidden_state.astype(jnp.float32)
        own_squares = jnp.sum(wide * wide, axis=1)
        gain = lax.dynamic_slice_in_dim(norm_gain[layer], column * width_dev, width_dev).astype(
            jnp.float32
        )
        gained = (wide * gain[None, :]).astype(jnp.bfloat16)
        partial_value = jnp.dot(gained, in_whole[layer], preferred_element_type=jnp.float32)
        squares = lax.psum(own_squares, "tp")
        summed_in = lax.psum_scatter(
            partial_value.astype(jnp.bfloat16), "tp", scatter_dimension=1, tiled=True
        ).astype(jnp.float32)
        row_scale = lax.rsqrt(squares / model_width + EPSILON)
        mixed_in = (summed_in * row_scale[:, None]).astype(jnp.bfloat16)
        before, before_labels = shifted((mixed_in[-span_reach:], labels[-span_reach:]), "sp", 1)
        padded = jnp.concatenate([before, mixed_in], axis=0).astype(jnp.float32)
        tags = jnp.concatenate([before_labels, labels], axis=0)
        pooled = span_pool(padded, tags, widths).astype(jnp.bfloat16)
        grouped = pooled.reshape(row_count, groups_dev, group_size)
        mixing = lax.dynamic_slice_in_dim(mix_pool[layer], column * groups_dev, groups_dev, 0)
        blended = jnp.einsum(
            "tgc,gcd->tgd", grouped, mixing, preferred_element_type=jnp.float32
        ).reshape(row_count, local)
        scale = lax.dynamic_slice_in_dim(pool_gain[layer], column * local, local).astype(
            jnp.float32
        )
        mixed = (blended * scale[None, :]).astype(jnp.bfloat16)
        full_mixed = lax.all_gather(mixed, "tp", axis=1, tiled=True)
        update = jnp.dot(full_mixed, out_whole[layer], preferred_element_type=jnp.float32)
        hidden_state = (wide + update).astype(jnp.bfloat16)
    return hidden_state


def solution(mesh):
    sp, tp = mesh.shape["sp"], mesh.shape["tp"]
    in_specs = (P("sp", "tp"), P("sp"), P(), P(None, "tp", "sp"), P(), P(), P(None, "sp", "tp"))

    def whole(stream, doc_ids, norm_gain, proj_in, mix_pool, pool_gain, proj_out):
        layers, _, channels = proj_in.shape
        group = mix_pool.shape[2]
        fits = (tp == 4 and sp == RING and layers == LAYERS and channels == sp * group and group == 128
                and mix_pool.shape[1] % 8 == 0 and stream.shape[0] % (sp * CHUNKS * 128) == 0)
        part = functools.partial(body, sp, tp) if fits else plain_body
        return jax.shard_map(part, mesh=mesh, in_specs=in_specs, out_specs=P("sp", "tp"), check_vma=False)(
            stream, doc_ids, norm_gain, proj_in, mix_pool, pool_gain, proj_out)

    return whole
```

```python
import functools

import jax
import jax.numpy as jnp
from jax import lax
from jax.experimental import pallas as pl
from jax.experimental.pallas import tpu as pltpu
from jax.sharding import PartitionSpec as P

EPSILON = 1e-06
HALO = 16
CHUNKS = 8
EDGE = 3
RING = 8
LAYERS = 3
MESH = pl.DeviceIdType.MESH
F32, BF16 = jnp.float32, jnp.bfloat16


def mixer(sp, tp, x_hbm, doc_ref, gains_ref, win_hbm, mix_ref, pgains_ref, wout_hbm, h,
          win, wout, gbuf, send1, own1, recv1, sum2, recv2, mixed, zbuf, hrecv,
          sq_own, sq_in, scale_ref, labels, before_labels, pos_ref, gain_ref, pgain_ref,
          xs, ws, ls, lr, ring_s, ring_r, sqs, sqr, s1, r1, s2, r2, s3, r3, hs, hr):
    layers, model_dev, chan_dev = win_hbm.shape
    tokens = h.shape[0]
    rows = tokens // CHUNKS
    channels = chan_dev * sp
    half = channels // 2
    group = mix_ref.shape[-1]
    own_groups = half // group
    model = model_dev * tp
    row_dev = wout_hbm.shape[1]
    last = CHUNKS - 1
    s, t = lax.axis_index("sp"), lax.axis_index("tp")
    core = lax.rem(t, 2)
    partner = t + 1 - 2 * core
    across = lax.rem(t + 2, tp)
    diagonal = lax.rem(partner + 2, tp)

    def place(device):
        z, y = device // 2, lax.rem(device, 2)
        return z * (1 - y) + (sp - 1 - z) * y

    def device_at(place):
        up = place // (sp // 2)
        return 2 * (place * (1 - up) + (sp - 1 - place) * up) + up

    here = place(s)
    after, before = device_at(lax.rem(here + 1, sp)), device_at(lax.rem(here + sp - 1, sp))
    following, leading = lax.rem(s + 1, sp), lax.rem(s + sp - 1, sp)

    def columns(device):
        return pl.ds(pl.multiple_of(device * chan_dev, chan_dev), chan_dev)

    def ring_view(layer, side, piece, source):
        if side == 0:
            part = model_dev // 2
            return win.at[layer, pl.ds(pl.multiple_of(piece * part, part), part), columns(source)]
        part = row_dev // 2
        return wout.at[layer, pl.ds(pl.multiple_of(source * row_dev + piece * part, part), part)]

    def ring_copy(layer, side, way, turn, back):
        hop = turn // 2 + back
        piece = lax.rem(turn + way, 2)
        origin = here - hop + sp if way == 0 else here + hop
        view = ring_view(layer, side, piece, device_at(lax.rem(origin, sp)))
        return pltpu.make_async_remote_copy(
            src_ref=view, dst_ref=view,
            send_sem=ring_s.at[layer, side, way, turn], recv_sem=ring_r.at[layer, side, way, turn],
            device_id={"sp": after if way == 0 else before}, device_id_type=MESH)

    turns = sp - 1
    items = 2 * layers

    def arrive(index):
        item, turn = index // turns, lax.rem(index, turns)
        layer, side = item // 2, lax.rem(item, 2)
        for which in range(2):
            @pl.when(side == which)
            def _():
                for way in range(2):
                    ring_copy(layer, which, way, turn, 1).wait_recv()

                @pl.when(turn < turns - 2)
                def _():
                    for way in range(2):
                        ring_copy(layer, which, way, turn + 2, 0).start()

                @pl.when((turn >= turns - 3) & (turn < turns - 1) & (item + 1 < items))
                def _():
                    for way in range(2):
                        ring_copy(layer + which, 1 - which, way, turn - (turns - 3), 0).start()

    def at(i):
        return pl.ds(pl.multiple_of(i * rows, rows), rows)

    def load_x(i):
        return pltpu.make_async_copy(x_hbm.at[at(i)], h.at[at(i)], xs.at[i])

    def load_w(layer, side):
        if side == 0:
            return pltpu.make_async_copy(win_hbm.at[layer], win.at[layer, :, columns(s)], ws.at[layer, side])
        return pltpu.make_async_copy(
            wout_hbm.at[layer], wout.at[layer, pl.ds(pl.multiple_of(s * row_dev, row_dev), row_dev)], ws.at[layer, side])

    load_w(0, 0).start()
    for i in range(CHUNKS):
        load_x(last - i).start()
    for layer in range(layers):
        for side in range(2):
            if layer + side > 0:
                load_w(layer, side).start()

    barrier = pltpu.get_barrier_semaphore()
    peers = ({"tp": partner}, {"tp": across}, {"tp": diagonal},
             {"sp": after}, {"sp": before}, {"sp": following}, {"sp": leading})
    for peer in peers:
        pl.semaphore_signal(barrier, inc=1, device_id=peer, device_id_type=MESH)
    own_gain = gains_ref[:, pl.ds(pl.multiple_of(t * model_dev, model_dev), model_dev)].astype(F32)
    own_pgain = pgains_ref[:, pl.ds(pl.multiple_of(core * half, half), half)].astype(F32)
    for layer in range(layers):
        gain_ref[layer] = own_gain[layer:layer + 1]
        pgain_ref[layer] = own_pgain[layer:layer + 1]
    load_w(0, 0).wait()
    pl.semaphore_wait(barrier, len(peers))
    for turn in range(2):
        for way in range(2):
            ring_copy(0, 0, way, turn, 0).start()
    reach = 2 * HALO
    label_copy = pltpu.make_async_remote_copy(
        src_ref=labels.at[pl.ds(tokens, reach)], dst_ref=before_labels, send_sem=ls, recv_sem=lr,
        device_id={"sp": following}, device_id_type=MESH)

    def distances(ext):
        run = (pltpu.roll(ext, 1, 0) == ext).astype(F32)
        size = 1
        while size < HALO:
            run = run + jnp.where(run == float(size), pltpu.roll(run, size, 0), 0.0)
            size *= 2
        return run[HALO:]

    def prepare():
        for i in range(EDGE):
            load_x(i).wait()
        for layer in range(layers):
            for side in range(2):
                if layer + side > 0:
                    load_w(layer, side).wait()
        documents = doc_ref[...].astype(F32)
        for j in range(tokens // 128):
            labels[pl.ds(reach + j * 128, 128)] = jnp.broadcast_to(documents[j:j + 1], (128, 128)).T
        label_copy.start()

    def measure():
        label_copy.wait()
        labels[pl.ds(0, reach)] = jnp.where(s == 0, -1.0, before_labels[...])
        pos_ref[pl.ds(0, HALO)] = distances(labels[pl.ds(0, reach)])

        @pl.loop(0, CHUNKS)
        def _(i):
            pos_ref[pl.ds(pl.multiple_of(HALO + i * rows, HALO), rows)] = distances(
                labels[pl.ds(pl.multiple_of(HALO + i * rows, HALO), rows + HALO)])

    def copy_sq(layer, i):
        par = lax.rem(layer, 2)
        return [pltpu.make_async_remote_copy(
            src_ref=sq_own.at[i], dst_ref=sq_in.at[j, par, i], send_sem=sqs.at[j, i], recv_sem=sqr.at[j, par, i],
            device_id={"tp": peer}, device_id_type=MESH)
            for j, peer in enumerate((partner, across, diagonal))]

    def copy1(i, lg):
        return pltpu.make_async_remote_copy(
            src_ref=send1.at[lg, i], dst_ref=recv1.at[lg, i], send_sem=s1.at[lg, i], recv_sem=r1.at[lg, i],
            device_id={"tp": partner}, device_id_type=MESH)

    def copy2(layer, i, lg):
        par = lax.rem(layer, 2)
        return pltpu.make_async_remote_copy(
            src_ref=sum2.at[lg, i], dst_ref=recv2.at[par, lg, i], send_sem=s2.at[lg, i], recv_sem=r2.at[par, lg, i],
            device_id={"tp": across}, device_id_type=MESH)

    def copy3(i, side, lg):
        view = mixed.at[i, :, pl.ds(pl.multiple_of(side * half + lg * group, group), group)]
        return pltpu.make_async_remote_copy(
            src_ref=view, dst_ref=view, send_sem=s3.at[lg, i], recv_sem=r3.at[lg, i],
            device_id={"tp": partner}, device_id_type=MESH)

    def halo_copy(layer, lg):
        return pltpu.make_async_remote_copy(
            src_ref=zbuf.at[lg, pl.ds(tokens, HALO)], dst_ref=hrecv.at[layer, lg],
            send_sem=hs.at[layer, lg], recv_sem=hr.at[layer, lg],
            device_id={"sp": following}, device_id_type=MESH)

    def groups_of(distance):
        return (device_at(lax.rem(here - distance + sp, sp)), device_at(lax.rem(here + distance, sp)))

    def owned(g):
        return g // own_groups == core

    def local(g):
        return lax.rem(g, own_groups)

    def gained_of(layer, i):
        wide = h[at(i)].astype(F32)
        squares = wide * wide
        lanes = squares[:, :128]
        for j in range(1, model_dev // 128):
            lanes = lanes + squares[:, j * 128:(j + 1) * 128]
        sq_own[i] = jnp.sum(lanes.T, axis=0, keepdims=True)
        gained = (wide * gain_ref[layer]).astype(BF16)
        for c in copy_sq(layer, i):
            c.start()
        return gained

    def deliver(i, g, value):
        @pl.when(owned(g))
        def _():
            own1[local(g), i] = value

        @pl.when(jnp.logical_not(owned(g)))
        def _():
            send1[local(g), i] = value
            copy1(i, local(g)).start()

    def project_groups(layer, distance, i):
        low, high = groups_of(distance)

        @pl.when(lax.rem(distance, sp // 2) == 0)
        def _():
            part = jnp.dot(gbuf[i], win[layer, :, columns(low)], preferred_element_type=F32).astype(BF16)
            deliver(i, low, part)

        @pl.when(lax.rem(distance, sp // 2) > 0)
        def _():
            weights = jnp.concatenate([win[layer, :, columns(low)], win[layer, :, columns(high)]], axis=1)
            part = jnp.dot(gbuf[i], weights, preferred_element_type=F32).astype(BF16)
            deliver(i, low, part[:, :group])
            deliver(i, high, part[:, group:])

    def project(layer, i):
        gained = gained_of(layer, i)
        other = pl.ds(pl.multiple_of((1 - core) * half, half), half)
        part = jnp.dot(gained, win[layer, :, other], preferred_element_type=F32).astype(BF16)
        for lg in range(own_groups):
            send1[lg, i] = part[:, lg * group:(lg + 1) * group]
            copy1(i, lg).start()
        mine = pl.ds(pl.multiple_of(core * half, half), half)
        part = jnp.dot(gained, win[layer, :, mine], preferred_element_type=F32).astype(BF16)
        for lg in range(own_groups):
            own1[lg, i] = part[:, lg * group:(lg + 1) * group]

    def add_up(layer, i, lg):
        sum2[lg, i] = (own1[lg, i].astype(F32) + recv1[lg, i].astype(F32)).astype(BF16)
        copy2(layer, i, lg).start()

    def each_group(distance, act):
        low, high = groups_of(distance)
        act(low)

        @pl.when(lax.rem(distance, sp // 2) > 0)
        def _():
            act(high)

    def join_groups(layer, distance, i):
        def act(g):
            @pl.when(owned(g))
            def _():
                copy1(i, local(g)).wait_recv()
                add_up(layer, i, local(g))

            @pl.when(jnp.logical_not(owned(g)))
            def _():
                copy1(i, local(g)).wait_send()
        each_group(distance, act)

    def join(layer, i):
        for lg in range(own_groups):
            copy1(i, lg).wait()
            add_up(layer, i, lg)

    def rescale(layer, i):
        par = lax.rem(layer, 2)
        total = sq_own[i]
        for j, c in enumerate(copy_sq(layer, i)):
            c.wait()
            total = total + sq_in[j, par, i]
        scale_ref[i] = jnp.broadcast_to(lax.rsqrt(total / model + EPSILON), (128, rows)).T

    def normalise(layer, i, lg):
        par = lax.rem(layer, 2)
        copy2(layer, i, lg).wait()
        summed = sum2[lg, i].astype(F32) + recv2[par, lg, i].astype(F32)
        zbuf[lg, pl.ds(pl.multiple_of(HALO + i * rows, HALO), rows)] = (summed * scale_ref[i]).astype(BF16)

        @pl.when(i == last)
        def _():
            halo_copy(layer, lg).start()

    def pool(layer, i, lg):
        @pl.when(i == 0)
        def _():
            halo_copy(layer, lg).wait()
            zbuf[lg, pl.ds(0, HALO)] = hrecv[layer, lg]

        wide_at = pl.ds(pl.multiple_of(i * rows, HALO), rows + HALO)
        pos = pos_ref[wide_at]
        z = zbuf[lg, wide_at].astype(F32)
        window = 2 ** (1 + lg % 4)
        total = z
        size = 1
        while size < window:
            total = total + jnp.where(pos >= size, pltpu.roll(total, size, 0), 0.0)
            size *= 2
        count = jnp.minimum(pos[HALO:] + 1.0, float(window))
        pooled = (total[HALO:] / count - z[HALO:]).astype(BF16)
        blended = jnp.dot(pooled, mix_ref[layer, core * own_groups + lg], preferred_element_type=F32)
        place_at = pl.ds(pl.multiple_of(core * half + lg * group, group), group)
        mixed[i, :, place_at] = (blended * pgain_ref[layer, :, lg * group:(lg + 1) * group]).astype(BF16)
        copy3(i, core, lg).start()

    def finish(layer, i):
        for lg in range(own_groups):
            copy3(i, core, lg).wait_send()
            copy3(i, 1 - core, lg).wait_recv()
        for j in range(2):
            cols = slice(j * (model_dev // 2), (j + 1) * (model_dev // 2))
            update = jnp.dot(mixed[i], wout[layer, :, cols], preferred_element_type=F32)
            h[at(i), cols] = (h[at(i), cols].astype(F32) + update).astype(BF16)


    spans = sp // 2 + 1

    @pl.loop(0, layers + 1)
    def _(layer):
        edge = EDGE + layer
        ending = layer // layers
        live = layer < layers
        slots = (spans + edge) * (1 - ending) + 2 * ending

        @pl.loop(0, slots)
        def _(q):
            later = layer - layer // 2
            turn = 2 * q - q // spans + later * (15 - (q + 9) // 10) + (layer // 2) * 16
            single = (q == spans - 1) | ((q == 0) & (layer > 0))
            count = CHUNKS - edge

            @pl.when(live & (q < spans))
            def _():
                @pl.loop(0, count)
                def _(j):
                    @pl.when(q == 0)
                    def _():
                        @pl.when(layer == 0)
                        def _():
                            load_x(last - j).wait()

                        gbuf[last - j] = gained_of(layer, last - j)

                    project_groups(layer, q, last - j)

                    @pl.when(j >= 2)
                    def _():
                        join_groups(layer, q, last - j + 2)

            @pl.when(q >= spans)
            def _():
                project(layer, edge - 1 - (q - spans))

            one = (q < 4) & (layer > 0)

            @pl.when(one | (q > spans + 2))
            def _():
                fresh = q // (spans + 3)
                finish(layer - 1 + fresh, (3 - q) * (1 - fresh) + (edge - (q - spans - 3)) * fresh)

            @pl.when(live & (q < spans))
            def _():
                for j in range(2):
                    join_groups(layer, q, edge + 1 - j)

            @pl.when(q >= spans)
            def _():
                join(layer, edge - 1 - (q - spans))

            @pl.when(live & (turn < turns * items))
            def _():
                arrive(turn)

            @pl.when((q == spans + 2) & live)
            def _():
                @pl.loop(0, CHUNKS - edge - 1)
                def _(j):
                    finish(layer, last - j)

            second = live & (turn + 1 < turns * items) & jnp.logical_not(single)

            @pl.when(second & (q == spans + 2))
            def _():
                arrive(turn + 1)

            @pl.when((layer == 0) & (q == 0))
            def _():
                prepare()

            @pl.when((layer == 0) & (q == 1))
            def _():
                measure()

            @pl.when(live & (q > 1) & (q < spans + 2))
            def _():
                distance = q - 2

                @pl.loop(0, CHUNKS - edge)
                def _(j):
                    @pl.when(distance == 0)
                    def _():
                        rescale(layer, last - j)

                    def act(g):
                        @pl.when(owned(g))
                        def _():
                            normalise(layer, last - j, local(g))
                    each_group(distance, act)

                @pl.loop(0, CHUNKS - edge - 1)
                def _(j):
                    def act(g):
                        for lg in range(own_groups):
                            @pl.when(owned(g) & (local(g) == lg))
                            def _():
                                pool(layer, last - j, lg)
                    each_group(distance, act)

            old = (q < 2) & (layer > 0)

            @pl.when(old | (q >= spans + 2))
            def _():
                fresh = q // (spans + 2)
                of = layer - 1 + fresh
                i = (1 - q) * (1 - fresh) + (edge - 1 - (q - 2 - spans)) * fresh
                rescale(of, i)
                for lg in range(own_groups):
                    normalise(of, i, lg)

                @pl.loop(0, 1 + (1 - fresh) * q)
                def _(j):
                    for lg in range(own_groups):
                        pool(of, i + 1 - j, lg)

            @pl.when(second & (q != spans + 2))
            def _():
                arrive(turn + 1)

    for i in range(2):
        finish(layers - 1, 1 - i)

    @pl.loop(0, layers)
    def _(layer):
        for side in range(2):
            for way in range(2):
                @pl.loop(0, turns)
                def _(turn):
                    ring_copy(layer, side, way, turn, 0).wait_send()


def body(sp, tp, stream, doc_ids, norm_gain, proj_in, mix_pool, pool_gain, proj_out):
    layers, model_dev, chan_dev = proj_in.shape
    tokens = stream.shape[0]
    rows = tokens // CHUNKS
    channels = chan_dev * sp
    half = channels // 2
    group = mix_pool.shape[-1]
    own = half // group
    dma, vmem = pltpu.SemaphoreType.DMA, pltpu.VMEM
    local, remote = pl.BlockSpec(memory_space=pltpu.VMEM), pl.BlockSpec(memory_space=pl.ANY)
    return pl.pallas_call(
        functools.partial(mixer, sp, tp),
        out_shape=pltpu.VMEM(stream.shape, BF16),
        in_specs=[remote, local, local, remote, local, local, remote],
        out_specs=local,
        scratch_shapes=[
            vmem((layers, model_dev, channels), BF16),
            vmem((layers, channels, model_dev), BF16),
            vmem((CHUNKS, rows, model_dev), BF16),
            vmem((own, CHUNKS, rows, group), BF16),
            vmem((own, CHUNKS, rows, group), BF16),
            vmem((own, CHUNKS, rows, group), BF16),
            vmem((own, CHUNKS, rows, group), BF16),
            vmem((2, own, CHUNKS, rows, group), BF16),
            vmem((CHUNKS, rows, channels), BF16),
            vmem((own, HALO + tokens, group), BF16),
            vmem((layers, own, HALO, group), BF16),
            vmem((CHUNKS, 1, rows), F32),
            vmem((3, 2, CHUNKS, 1, rows), F32),
            vmem((CHUNKS, rows, 128), F32),
            vmem((2 * HALO + tokens, 128), F32),
            vmem((2 * HALO, 128), F32),
            vmem((HALO + tokens, 128), F32),
            vmem((layers, 1, model_dev), F32),
            vmem((layers, 1, half), F32),
            dma((CHUNKS,)), dma((layers, 2)),
            dma, dma,
            dma((layers, 2, 2, sp - 1)), dma((layers, 2, 2, sp - 1)),
            dma((3, CHUNKS)), dma((3, 2, CHUNKS)),
            dma((own, CHUNKS)), dma((own, CHUNKS)),
            dma((own, CHUNKS)), dma((2, own, CHUNKS)),
            dma((own, CHUNKS)), dma((own, CHUNKS)),
            dma((layers, own)), dma((layers, own)),
        ],
        compiler_params=pltpu.CompilerParams(
            collective_id=0, has_side_effects=True, vmem_limit_bytes=56 * 2**20),
    )(stream, doc_ids.reshape(-1, 128), norm_gain, proj_in, mix_pool, pool_gain, proj_out)


span_reach = 15


def shifted(value, axis, steps):
    count = lax.axis_size(axis)
    initial, last = (max(0, -steps), min(count, count - steps))
    return lax.ppermute(value, axis, [(source, source + steps) for source in range(initial, last)])


def span_pool(padded, labels, widths):
    kept = padded.shape[0] - span_reach
    own_label = labels[span_reach:]
    summed = jnp.zeros((kept, padded.shape[1]), jnp.float32)
    counted = jnp.zeros((kept, padded.shape[1]), jnp.float32)
    for offset in range(span_reach + 1):
        first = span_reach - offset
        member = (labels[first : first + kept] == own_label)[:, None] & (offset < widths)[None, :]
        factor = member.astype(jnp.float32)
        summed = summed + padded[first : first + kept] * factor
        counted = counted + factor
    return summed / counted - padded[span_reach:]


def plain_body(stream, doc_ids, norm_gain, proj_in, mix_pool, pool_gain, proj_out):
    width_dev = stream.shape[1]
    tp_count = lax.axis_size("tp")
    model_width = width_dev * tp_count
    group_size = mix_pool.shape[2]
    channels = proj_in.shape[2] * lax.axis_size("sp")
    local = channels // tp_count
    groups_dev = local // group_size
    column = lax.axis_index("tp")
    chan_ids = column * local + jnp.arange(local, dtype=jnp.int32)
    widths = jnp.left_shift(jnp.int32(2), chan_ids // group_size % 4)
    labels = (doc_ids + 1).astype(jnp.bfloat16)
    hidden_state = stream
    layer_count = proj_in.shape[0]
    in_whole, out_whole = (
        lax.all_gather(proj_in, "sp", axis=2, tiled=True),
        lax.all_gather(proj_out, "sp", axis=1, tiled=True),
    )
    for layer in range(layer_count):
        row_count = hidden_state.shape[0]
        wide = hidden_state.astype(jnp.float32)
        own_squares = jnp.sum(wide * wide, axis=1)
        gain = lax.dynamic_slice_in_dim(norm_gain[layer], column * width_dev, width_dev).astype(
            jnp.float32
        )
        gained = (wide * gain[None, :]).astype(jnp.bfloat16)
        partial_value = jnp.dot(gained, in_whole[layer], preferred_element_type=jnp.float32)
        squares = lax.psum(own_squares, "tp")
        summed_in = lax.psum_scatter(
            partial_value.astype(jnp.bfloat16), "tp", scatter_dimension=1, tiled=True
        ).astype(jnp.float32)
        row_scale = lax.rsqrt(squares / model_width + EPSILON)
        mixed_in = (summed_in * row_scale[:, None]).astype(jnp.bfloat16)
        before, before_labels = shifted((mixed_in[-span_reach:], labels[-span_reach:]), "sp", 1)
        padded = jnp.concatenate([before, mixed_in], axis=0).astype(jnp.float32)
        tags = jnp.concatenate([before_labels, labels], axis=0)
        pooled = span_pool(padded, tags, widths).astype(jnp.bfloat16)
        grouped = pooled.reshape(row_count, groups_dev, group_size)
        mixing = lax.dynamic_slice_in_dim(mix_pool[layer], column * groups_dev, groups_dev, 0)
        blended = jnp.einsum(
            "tgc,gcd->tgd", grouped, mixing, preferred_element_type=jnp.float32
        ).reshape(row_count, local)
        scale = lax.dynamic_slice_in_dim(pool_gain[layer], column * local, local).astype(
            jnp.float32
        )
        mixed = (blended * scale[None, :]).astype(jnp.bfloat16)
        full_mixed = lax.all_gather(mixed, "tp", axis=1, tiled=True)
        update = jnp.dot(full_mixed, out_whole[layer], preferred_element_type=jnp.float32)
        hidden_state = (wide + update).astype(jnp.bfloat16)
    return hidden_state


def solution(mesh):
    sp, tp = mesh.shape["sp"], mesh.shape["tp"]
    in_specs = (P("sp", "tp"), P("sp"), P(), P(None, "tp", "sp"), P(), P(), P(None, "sp", "tp"))

    def whole(stream, doc_ids, norm_gain, proj_in, mix_pool, pool_gain, proj_out):
        layers, _, channels = proj_in.shape
        group = mix_pool.shape[2]
        fits = (tp == 4 and sp == RING and layers == LAYERS and channels == sp * group and group == 128
                and mix_pool.shape[1] % 8 == 0 and stream.shape[0] % (sp * CHUNKS * 128) == 0)
        part = functools.partial(body, sp, tp) if fits else plain_body
        return jax.shard_map(part, mesh=mesh, in_specs=in_specs, out_specs=P("sp", "tp"), check_vma=False)(
            stream, doc_ids, norm_gain, proj_in, mix_pool, pool_gain, proj_out)

    return whole
```

```python
import functools

import jax
import jax.numpy as jnp
from jax import lax
from jax.experimental import pallas as pl
from jax.experimental.pallas import tpu as pltpu
from jax.sharding import PartitionSpec as P

EPSILON = 1e-06
HALO = 16
CHUNKS = 8
EDGE = 2
RING = 8
LAYERS = 3
MESH = pl.DeviceIdType.MESH
F32, BF16 = jnp.float32, jnp.bfloat16


def mixer(sp, tp, x_hbm, doc_ref, gains_ref, win_hbm, mix_ref, pgains_ref, wout_hbm, h,
          win, wout, gbuf, send1, own1, recv1, sum2, recv2, mixed, zbuf, hrecv,
          sq_own, sq_in, scale_ref, labels, before_labels, pos_ref, gain_ref, pgain_ref,
          xs, ws, ls, lr, ring_s, ring_r, sqs, sqr, s1, r1, s2, r2, s3, r3, hs, hr):
    layers, model_dev, chan_dev = win_hbm.shape
    tokens = h.shape[0]
    rows = tokens // CHUNKS
    channels = chan_dev * sp
    half = channels // 2
    group = mix_ref.shape[-1]
    own_groups = half // group
    model = model_dev * tp
    row_dev = wout_hbm.shape[1]
    last = CHUNKS - 1
    s, t = lax.axis_index("sp"), lax.axis_index("tp")
    core = lax.rem(t, 2)
    partner = t + 1 - 2 * core
    across = lax.rem(t + 2, tp)
    diagonal = lax.rem(partner + 2, tp)

    def place(device):
        z, y = device // 2, lax.rem(device, 2)
        return z * (1 - y) + (sp - 1 - z) * y

    def device_at(place):
        up = place // (sp // 2)
        return 2 * (place * (1 - up) + (sp - 1 - place) * up) + up

    here = place(s)
    after, before = device_at(lax.rem(here + 1, sp)), device_at(lax.rem(here + sp - 1, sp))
    following, leading = lax.rem(s + 1, sp), lax.rem(s + sp - 1, sp)

    def columns(device):
        return pl.ds(pl.multiple_of(device * chan_dev, chan_dev), chan_dev)

    def ring_view(layer, side, piece, source):
        if side == 0:
            part = model_dev // 2
            return win.at[layer, pl.ds(pl.multiple_of(piece * part, part), part), columns(source)]
        part = row_dev // 2
        return wout.at[layer, pl.ds(pl.multiple_of(source * row_dev + piece * part, part), part)]

    def ring_copy(layer, side, way, turn, back):
        hop = turn // 2 + back
        piece = lax.rem(turn + way, 2)
        origin = here - hop + sp if way == 0 else here + hop
        view = ring_view(layer, side, piece, device_at(lax.rem(origin, sp)))
        return pltpu.make_async_remote_copy(
            src_ref=view, dst_ref=view,
            send_sem=ring_s.at[way, turn], recv_sem=ring_r.at[way, turn],
            device_id={"sp": after if way == 0 else before}, device_id_type=MESH)

    turns = sp - 1
    items = 2 * layers

    def arrive(index):
        item, turn = index // turns, lax.rem(index, turns)
        layer, side = item // 2, lax.rem(item, 2)
        for which in range(2):
            @pl.when(side == which)
            def _():
                for way in range(2):
                    ring_copy(layer, which, way, turn, 1).wait_recv()

                @pl.when((turn < turns - 2) & (item > 0))
                def _():
                    for way in range(2):
                        ring_copy(layer + which - 1, 1 - which, way, turn + 2, 0).wait_send()

                @pl.when(turn < turns - 2)
                def _():
                    for way in range(2):
                        ring_copy(layer, which, way, turn + 2, 0).start()

                @pl.when((turn >= turns - 3) & (turn < turns - 1) & (item + 1 < items))
                def _():
                    for way in range(2):
                        ring_copy(layer, which, way, turn - (turns - 3), 0).wait_send()
                        ring_copy(layer + which, 1 - which, way, turn - (turns - 3), 0).start()

    def at(i):
        return pl.ds(pl.multiple_of(i * rows, rows), rows)

    def load_x(i):
        return pltpu.make_async_copy(x_hbm.at[at(i)], h.at[at(i)], xs.at[i])

    def load_w(layer, side):
        if side == 0:
            return pltpu.make_async_copy(win_hbm.at[layer], win.at[layer, :, columns(s)], ws.at[layer, side])
        return pltpu.make_async_copy(
            wout_hbm.at[layer], wout.at[layer, pl.ds(pl.multiple_of(s * row_dev, row_dev), row_dev)], ws.at[layer, side])

    load_w(0, 0).start()
    for i in range(CHUNKS):
        load_x(last - i).start()
    for layer in range(layers):
        for side in range(2):
            if layer + side > 0:
                load_w(layer, side).start()

    barrier = pltpu.get_barrier_semaphore()
    peers = ({"tp": partner}, {"tp": across}, {"tp": diagonal},
             {"sp": after}, {"sp": before}, {"sp": following}, {"sp": leading})
    for peer in peers:
        pl.semaphore_signal(barrier, inc=1, device_id=peer, device_id_type=MESH)
    own_gain = gains_ref[:, pl.ds(pl.multiple_of(t * model_dev, model_dev), model_dev)].astype(F32)
    own_pgain = pgains_ref[:, pl.ds(pl.multiple_of(core * half, half), half)].astype(F32)
    for layer in range(layers):
        gain_ref[layer] = own_gain[layer:layer + 1]
        pgain_ref[layer] = own_pgain[layer:layer + 1]
    load_w(0, 0).wait()
    pl.semaphore_wait(barrier, len(peers))
    for turn in range(2):
        for way in range(2):
            ring_copy(0, 0, way, turn, 0).start()
    reach = 2 * HALO
    label_copy = pltpu.make_async_remote_copy(
        src_ref=labels.at[pl.ds(tokens, reach)], dst_ref=before_labels, send_sem=ls, recv_sem=lr,
        device_id={"sp": following}, device_id_type=MESH)

    def distances(ext):
        run = (pltpu.roll(ext, 1, 0) == ext).astype(F32)
        size = 1
        while size < HALO:
            run = run + jnp.where(run == float(size), pltpu.roll(run, size, 0), 0.0)
            size *= 2
        return run[HALO:]

    def prepare():
        for layer in range(layers):
            for side in range(2):
                if layer + side > 0:
                    load_w(layer, side).wait()
        documents = doc_ref[...].astype(F32)
        for j in range(tokens // 128):
            labels[pl.ds(reach + j * 128, 128)] = jnp.broadcast_to(documents[j:j + 1], (128, 128)).T
        label_copy.start()

    def measure():
        label_copy.wait()
        labels[pl.ds(0, reach)] = jnp.where(s == 0, -1.0, before_labels[...])
        pos_ref[pl.ds(0, HALO)] = distances(labels[pl.ds(0, reach)])

        @pl.loop(0, CHUNKS)
        def _(i):
            pos_ref[pl.ds(pl.multiple_of(HALO + i * rows, HALO), rows)] = distances(
                labels[pl.ds(pl.multiple_of(HALO + i * rows, HALO), rows + HALO)])

    def copy_sq(layer, i):
        par = lax.rem(layer, 2)
        return [pltpu.make_async_remote_copy(
            src_ref=sq_own.at[i], dst_ref=sq_in.at[par, i, j], send_sem=sqs.at[i], recv_sem=sqr.at[par, i],
            device_id={"tp": peer}, device_id_type=MESH)
            for j, peer in enumerate((partner, across, diagonal))]

    def copy1(i, lg):
        return pltpu.make_async_remote_copy(
            src_ref=send1.at[lg, i], dst_ref=recv1.at[lg, i], send_sem=s1.at[i], recv_sem=r1.at[lg, i],
            device_id={"tp": partner}, device_id_type=MESH)

    def copy2(layer, i, lg):
        par = lax.rem(layer, 2)
        return pltpu.make_async_remote_copy(
            src_ref=sum2.at[lg, i], dst_ref=recv2.at[par, lg, i], send_sem=s2.at[i], recv_sem=r2.at[par, lg, i],
            device_id={"tp": across}, device_id_type=MESH)

    def copy3(i, side, lg):
        view = mixed.at[i, :, pl.ds(pl.multiple_of(side * half + lg * group, group), group)]
        return pltpu.make_async_remote_copy(
            src_ref=view, dst_ref=view, send_sem=s3.at[i], recv_sem=r3.at[i],
            device_id={"tp": partner}, device_id_type=MESH)

    def halo_copy(layer, lg):
        return pltpu.make_async_remote_copy(
            src_ref=zbuf.at[lg, pl.ds(tokens, HALO)], dst_ref=hrecv.at[layer, lg],
            send_sem=hs.at[layer], recv_sem=hr.at[layer],
            device_id={"sp": following}, device_id_type=MESH)

    def groups_of(distance):
        return (device_at(lax.rem(here - distance + sp, sp)), device_at(lax.rem(here + distance, sp)))

    def owned(g):
        return g // own_groups == core

    def local(g):
        return lax.rem(g, own_groups)

    def gained_of(layer, i):
        wide = h[at(i)].astype(F32)
        squares = wide * wide
        lanes = squares[:, :128]
        for j in range(1, model_dev // 128):
            lanes = lanes + squares[:, j * 128:(j + 1) * 128]
        sq_own[i] = jnp.sum(lanes.T, axis=0, keepdims=True)
        gained = (wide * gain_ref[layer]).astype(BF16)
        for c in copy_sq(layer, i):
            c.start()
        return gained

    def deliver(i, g, value):
        @pl.when(owned(g))
        def _():
            own1[local(g), i] = value

        @pl.when(jnp.logical_not(owned(g)))
        def _():
            send1[local(g), i] = value
            copy1(i, local(g)).start()

    def project_groups(layer, distance, i):
        low, high = groups_of(distance)

        @pl.when(lax.rem(distance, sp // 2) == 0)
        def _():
            part = jnp.dot(gbuf[i], win[layer, :, columns(low)], preferred_element_type=F32).astype(BF16)
            deliver(i, low, part)

        @pl.when(lax.rem(distance, sp // 2) > 0)
        def _():
            weights = jnp.concatenate([win[layer, :, columns(low)], win[layer, :, columns(high)]], axis=1)
            part = jnp.dot(gbuf[i], weights, preferred_element_type=F32).astype(BF16)
            deliver(i, low, part[:, :group])
            deliver(i, high, part[:, group:])

    def project(layer, i):
        @pl.when(layer > 0)
        def _():
            gbuf[i] = gained_of(layer, i)

        gained = gbuf[i]
        other = pl.ds(pl.multiple_of((1 - core) * half, half), half)
        part = jnp.dot(gained, win[layer, :, other], preferred_element_type=F32).astype(BF16)
        for lg in range(own_groups):
            @pl.when((layer > 0) | ((1 - core) * own_groups + lg != s))
            def _():
                send1[lg, i] = part[:, lg * group:(lg + 1) * group]
                copy1(i, lg).start()
        mine = pl.ds(pl.multiple_of(core * half, half), half)
        part = jnp.dot(gained, win[layer, :, mine], preferred_element_type=F32).astype(BF16)
        for lg in range(own_groups):
            own1[lg, i] = part[:, lg * group:(lg + 1) * group]

    def add_up(layer, i, lg):
        sum2[lg, i] = (own1[lg, i].astype(F32) + recv1[lg, i].astype(F32)).astype(BF16)
        copy2(layer, i, lg).start()

    def each_group(distance, act):
        low, high = groups_of(distance)
        act(low)

        @pl.when(lax.rem(distance, sp // 2) > 0)
        def _():
            act(high)

    def join_groups(layer, distance, i):
        def act(g):
            @pl.when(owned(g))
            def _():
                copy1(i, local(g)).wait_recv()
                add_up(layer, i, local(g))

        each_group(distance, act)

    def join(layer, i):
        for lg in range(own_groups):
            @pl.when((layer > 0) | (core * own_groups + lg != s))
            def _():
                copy1(i, lg).wait_recv()
                add_up(layer, i, lg)

    def rescale(layer, i):
        par = lax.rem(layer, 2)
        pltpu.make_async_remote_copy(
            src_ref=sq_in.at[par, i], dst_ref=sq_in.at[par, i], send_sem=sqs.at[i], recv_sem=sqr.at[par, i],
            device_id={"tp": partner}, device_id_type=MESH).wait()
        total = sq_own[i]
        for j in range(3):
            total = total + sq_in[par, i, j]
        scale_ref[i] = jnp.broadcast_to(lax.rsqrt(total / model + EPSILON), (128, rows)).T

    def normalise(layer, i, lg):
        par = lax.rem(layer, 2)
        copy2(layer, i, lg).wait_recv()
        summed = sum2[lg, i].astype(F32) + recv2[par, lg, i].astype(F32)
        zbuf[lg, pl.ds(pl.multiple_of(HALO + i * rows, HALO), rows)] = (summed * scale_ref[i]).astype(BF16)

    def pool(layer, i, lg):
        wide_at = pl.ds(pl.multiple_of(i * rows, HALO), rows + HALO)
        pos = pos_ref[wide_at]
        z = zbuf[lg, wide_at].astype(F32)
        window = 2 ** (1 + lg % 4)
        total = z
        size = 1
        while size < window:
            total = total + jnp.where(pos >= size, pltpu.roll(total, size, 0), 0.0)
            size *= 2
        count = jnp.minimum(pos[HALO:] + 1.0, float(window))
        pooled = (total[HALO:] / count - z[HALO:]).astype(BF16)
        blended = jnp.dot(pooled, mix_ref[layer, core * own_groups + lg], preferred_element_type=F32)
        place_at = pl.ds(pl.multiple_of(core * half + lg * group, group), group)
        mixed[i, :, place_at] = (blended * pgain_ref[layer, :, lg * group:(lg + 1) * group]).astype(BF16)
        copy3(i, core, lg).start()

    def side_of(i, side):
        return mixed.at[i, :, pl.ds(pl.multiple_of(side * half, half), half)]

    def take_halo(layer):
        pltpu.make_async_remote_copy(
            src_ref=zbuf.at[:, pl.ds(tokens, HALO)], dst_ref=hrecv.at[layer], send_sem=hs.at[layer], recv_sem=hr.at[layer],
            device_id={"sp": following}, device_id_type=MESH).wait()
        zbuf[:, pl.ds(0, HALO)] = hrecv[layer]

    def finish(layer, i):
        for src, dst, sems in ((send1.at[:, i], recv1.at[:, i], s1), (sum2.at[:, i], recv2.at[0, :, i], s2),
                               (side_of(i, core), side_of(i, core), s3)):
            pltpu.make_async_remote_copy(
                src_ref=src, dst_ref=dst, send_sem=sems.at[i], recv_sem=r3.at[i],
                device_id={"tp": partner}, device_id_type=MESH).wait_send()
        pltpu.make_async_remote_copy(
            src_ref=side_of(i, 1 - core), dst_ref=side_of(i, 1 - core), send_sem=s3.at[i], recv_sem=r3.at[i],
            device_id={"tp": partner}, device_id_type=MESH).wait_recv()
        for j in range(2):
            cols = slice(j * (model_dev // 2), (j + 1) * (model_dev // 2))
            update = jnp.dot(mixed[i], wout[layer, :, cols], preferred_element_type=F32)
            h[at(i), cols] = (h[at(i), cols].astype(F32) + update).astype(BF16)


    spans = sp // 2 + 1

    @pl.loop(0, layers + 1)
    def _(layer):
        edge = EDGE + layer
        ending = layer // layers
        live = layer < layers
        slots = (spans + edge) * (1 - ending) + 2 * ending

        @pl.loop(0, slots)
        def _(q):
            def past(k):
                return (q + 15 - k) // 16

            middle, final = lax.rem(layer, 2), layer // 2
            turn = 2 * q + middle * (14 - past(4)) + final * (29 - past(2) - past(3) - past(4))
            opening = (q == 0) & (layer > 0)
            single = opening | ((middle == 1) & (q == 4)) | ((final == 1) & (q > 1) & (q < 5))
            everything = ((q == 0) & (layer == 0)).astype(jnp.int32)
            count = CHUNKS - edge + edge * everything

            @pl.when(live & (q < spans))
            def _():
                @pl.loop(0, count)
                def _(j):
                    @pl.when(q == 0)
                    def _():
                        @pl.when(layer == 0)
                        def _():
                            load_x(last - j).wait()

                        @pl.when(layer == 1)
                        def _():
                            finish(layer - 1, last - j)

                        gbuf[last - j] = gained_of(layer, last - j)

                    project_groups(layer, q, last - j)

                    @pl.when(j >= 2)
                    def _():
                        join_groups(layer, q, last - j + 2)

                    @pl.when(opening & (j == 2))
                    def _():
                        arrive(turn)

            @pl.when(q >= spans)
            def _():
                project(layer, edge - 1 - (q - spans))

            one = (layer > 0) & (((ending == 1) & (q < 2)) | (live & (q > 0) & (q < 5) & (q + edge > 4)))

            @pl.when(one | (q > spans + 2))
            def _():
                fresh = q // (spans + 3)
                finish(layer - 1 + fresh, (4 - ending - q) * (1 - fresh) + (edge - (q - spans - 3)) * fresh)

            @pl.when(live & (q < spans))
            def _():
                for j in range(2):
                    join_groups(layer, q, CHUNKS - count + 1 - j)

            @pl.when(q >= spans)
            def _():
                join(layer, edge - 1 - (q - spans))

            after_join = turn + opening.astype(jnp.int32)

            @pl.when(live & (after_join < turns * items))
            def _():
                arrive(after_join)

            @pl.when((layer == 0) & (q == 0))
            def _():
                prepare()

            @pl.when((layer == 0) & (q == 1))
            def _():
                measure()

            @pl.when(live & (q > 1) & (q < spans + 2))
            def _():
                distance = q - 2

                @pl.loop(0, CHUNKS - edge)
                def _(j):
                    @pl.when(distance == 0)
                    def _():
                        rescale(layer, last - j)

                    def act(g):
                        @pl.when(owned(g))
                        def _():
                            normalise(layer, last - j, local(g))

                            @pl.when(j == 0)
                            def _():
                                halo_copy(layer, local(g)).start()
                    each_group(distance, act)

                @pl.loop(0, CHUNKS - edge - 1)
                def _(j):
                    def act(g):
                        for lg in range(own_groups):
                            @pl.when(owned(g) & (local(g) == lg))
                            def _():
                                pool(layer, last - j, lg)
                    each_group(distance, act)

            old = (layer > 0) & (((ending == 1) & (q < 2)) | (live & (q == 1)))

            @pl.when(old | (q >= spans + 2))
            def _():
                fresh = q // (spans + 2)
                of = layer - 1 + fresh
                first = (1 - q * ending) * (1 - fresh) + (edge - 1 - (q - 2 - spans)) * fresh

                @pl.loop(0, 1 + (1 - fresh) * (1 - ending))
                def _(j):
                    i = first - j
                    rescale(of, i)

                    @pl.when(i == 0)
                    def _():
                        take_halo(of)

                    for lg in range(own_groups):
                        normalise(of, i, lg)
                        pool(of, i + 1, lg)

                        @pl.when(i == 0)
                        def _():
                            pool(of, i, lg)

            @pl.when(live & (turn + 1 < turns * items) & jnp.logical_not(single))
            def _():
                arrive(turn + 1)

            @pl.when((layer > 0) & live & (q == slots - 1))
            def _():
                @pl.loop(0, CHUNKS - edge - 1)
                def _(j):
                    finish(layer, last - j)

    for i in range(2):
        finish(layers - 1, 1 - i)

    for way in range(2):
        for turn in range(turns):
            ring_copy(layers - 1, 1, way, turn, 0).wait_send()


def body(sp, tp, stream, doc_ids, norm_gain, proj_in, mix_pool, pool_gain, proj_out):
    layers, model_dev, chan_dev = proj_in.shape
    tokens = stream.shape[0]
    rows = tokens // CHUNKS
    channels = chan_dev * sp
    half = channels // 2
    group = mix_pool.shape[-1]
    own = half // group
    dma, vmem = pltpu.SemaphoreType.DMA, pltpu.VMEM
    local, remote = pl.BlockSpec(memory_space=pltpu.VMEM), pl.BlockSpec(memory_space=pl.ANY)
    return pl.pallas_call(
        functools.partial(mixer, sp, tp),
        out_shape=pltpu.VMEM(stream.shape, BF16),
        in_specs=[remote, local, local, remote, local, local, remote],
        out_specs=local,
        scratch_shapes=[
            vmem((layers, model_dev, channels), BF16),
            vmem((layers, channels, model_dev), BF16),
            vmem((CHUNKS, rows, model_dev), BF16),
            vmem((own, CHUNKS, rows, group), BF16),
            vmem((own, CHUNKS, rows, group), BF16),
            vmem((own, CHUNKS, rows, group), BF16),
            vmem((own, CHUNKS, rows, group), BF16),
            vmem((2, own, CHUNKS, rows, group), BF16),
            vmem((CHUNKS, rows, channels), BF16),
            vmem((own, HALO + tokens, group), BF16),
            vmem((layers, own, HALO, group), BF16),
            vmem((CHUNKS, 1, rows), F32),
            vmem((2, CHUNKS, 3, 1, rows), F32),
            vmem((CHUNKS, rows, 128), F32),
            vmem((2 * HALO + tokens, 128), F32),
            vmem((2 * HALO, 128), F32),
            vmem((HALO + tokens, 128), F32),
            vmem((layers, 1, model_dev), F32),
            vmem((layers, 1, half), F32),
            dma((CHUNKS,)), dma((layers, 2)),
            dma, dma,
            dma((2, sp - 1)), dma((2, sp - 1)),
            dma((CHUNKS,)), dma((2, CHUNKS)),
            dma((CHUNKS,)), dma((own, CHUNKS)),
            dma((CHUNKS,)), dma((2, own, CHUNKS)),
            dma((CHUNKS,)), dma((CHUNKS,)),
            dma((layers,)), dma((layers,)),
        ],
        compiler_params=pltpu.CompilerParams(
            collective_id=0, has_side_effects=True, vmem_limit_bytes=56 * 2**20),
    )(stream, doc_ids.reshape(-1, 128), norm_gain, proj_in, mix_pool, pool_gain, proj_out)


span_reach = 15


def shifted(value, axis, steps):
    count = lax.axis_size(axis)
    initial, last = (max(0, -steps), min(count, count - steps))
    return lax.ppermute(value, axis, [(source, source + steps) for source in range(initial, last)])


def span_pool(padded, labels, widths):
    kept = padded.shape[0] - span_reach
    own_label = labels[span_reach:]
    summed = jnp.zeros((kept, padded.shape[1]), jnp.float32)
    counted = jnp.zeros((kept, padded.shape[1]), jnp.float32)
    for offset in range(span_reach + 1):
        first = span_reach - offset
        member = (labels[first : first + kept] == own_label)[:, None] & (offset < widths)[None, :]
        factor = member.astype(jnp.float32)
        summed = summed + padded[first : first + kept] * factor
        counted = counted + factor
    return summed / counted - padded[span_reach:]


def plain_body(stream, doc_ids, norm_gain, proj_in, mix_pool, pool_gain, proj_out):
    width_dev = stream.shape[1]
    tp_count = lax.axis_size("tp")
    model_width = width_dev * tp_count
    group_size = mix_pool.shape[2]
    channels = proj_in.shape[2] * lax.axis_size("sp")
    local = channels // tp_count
    groups_dev = local // group_size
    column = lax.axis_index("tp")
    chan_ids = column * local + jnp.arange(local, dtype=jnp.int32)
    widths = jnp.left_shift(jnp.int32(2), chan_ids // group_size % 4)
    labels = (doc_ids + 1).astype(jnp.bfloat16)
    hidden_state = stream
    layer_count = proj_in.shape[0]
    in_whole, out_whole = (
        lax.all_gather(proj_in, "sp", axis=2, tiled=True),
        lax.all_gather(proj_out, "sp", axis=1, tiled=True),
    )
    for layer in range(layer_count):
        row_count = hidden_state.shape[0]
        wide = hidden_state.astype(jnp.float32)
        own_squares = jnp.sum(wide * wide, axis=1)
        gain = lax.dynamic_slice_in_dim(norm_gain[layer], column * width_dev, width_dev).astype(
            jnp.float32
        )
        gained = (wide * gain[None, :]).astype(jnp.bfloat16)
        partial_value = jnp.dot(gained, in_whole[layer], preferred_element_type=jnp.float32)
        squares = lax.psum(own_squares, "tp")
        summed_in = lax.psum_scatter(
            partial_value.astype(jnp.bfloat16), "tp", scatter_dimension=1, tiled=True
        ).astype(jnp.float32)
        row_scale = lax.rsqrt(squares / model_width + EPSILON)
        mixed_in = (summed_in * row_scale[:, None]).astype(jnp.bfloat16)
        before, before_labels = shifted((mixed_in[-span_reach:], labels[-span_reach:]), "sp", 1)
        padded = jnp.concatenate([before, mixed_in], axis=0).astype(jnp.float32)
        tags = jnp.concatenate([before_labels, labels], axis=0)
        pooled = span_pool(padded, tags, widths).astype(jnp.bfloat16)
        grouped = pooled.reshape(row_count, groups_dev, group_size)
        mixing = lax.dynamic_slice_in_dim(mix_pool[layer], column * groups_dev, groups_dev, 0)
        blended = jnp.einsum(
            "tgc,gcd->tgd", grouped, mixing, preferred_element_type=jnp.float32
        ).reshape(row_count, local)
        scale = lax.dynamic_slice_in_dim(pool_gain[layer], column * local, local).astype(
            jnp.float32
        )
        mixed = (blended * scale[None, :]).astype(jnp.bfloat16)
        full_mixed = lax.all_gather(mixed, "tp", axis=1, tiled=True)
        update = jnp.dot(full_mixed, out_whole[layer], preferred_element_type=jnp.float32)
        hidden_state = (wide + update).astype(jnp.bfloat16)
    return hidden_state


def solution(mesh):
    sp, tp = mesh.shape["sp"], mesh.shape["tp"]
    in_specs = (P("sp", "tp"), P("sp"), P(), P(None, "tp", "sp"), P(), P(), P(None, "sp", "tp"))

    def whole(stream, doc_ids, norm_gain, proj_in, mix_pool, pool_gain, proj_out):
        layers, _, channels = proj_in.shape
        group = mix_pool.shape[2]
        fits = (tp == 4 and sp == RING and layers == LAYERS and channels == sp * group and group == 128
                and mix_pool.shape[1] % 8 == 0 and stream.shape[0] % (sp * CHUNKS * 128) == 0)
        part = functools.partial(body, sp, tp) if fits else plain_body
        return jax.shard_map(part, mesh=mesh, in_specs=in_specs, out_specs=P("sp", "tp"), check_vma=False)(
            stream, doc_ids, norm_gain, proj_in, mix_pool, pool_gain, proj_out)

    return whole
```

```python
import functools

import jax
import jax.numpy as jnp
from jax import lax
from jax.experimental import pallas as pl
from jax.experimental.pallas import tpu as pltpu
from jax.sharding import PartitionSpec as P

EPSILON = 1e-06
HALO = 16
CHUNKS = 8
EDGE = 2
RING = 8
LAYERS = 3
MESH = pl.DeviceIdType.MESH
F32, BF16 = jnp.float32, jnp.bfloat16


def mixer(sp, tp, x_hbm, doc_ref, gains_ref, win_hbm, mix_ref, pgains_ref, wout_hbm, h,
          win, wout, gbuf, send1, own1, recv1, sum2, recv2, mixed, zbuf, hrecv,
          sq_own, sq_in, scale_ref, labels, before_labels, pos_ref, inverse, gain_ref, pgain_ref,
          xs, ws, ls, lr, ring_s, ring_r, sqs, sqr, s1, r1, s2, r2, rh, s3, r3, hs, hr):
    layers, model_dev, chan_dev = win_hbm.shape
    tokens = h.shape[0]
    rows = tokens // CHUNKS
    channels = chan_dev * sp
    half = channels // 2
    group = mix_ref.shape[-1]
    own_groups = half // group
    model = model_dev * tp
    row_dev = wout_hbm.shape[1]
    last = CHUNKS - 1
    s, t = lax.axis_index("sp"), lax.axis_index("tp")
    core = lax.rem(t, 2)
    partner = t + 1 - 2 * core
    across = lax.rem(t + 2, tp)
    diagonal = lax.rem(partner + 2, tp)

    def place(device):
        z, y = device // 2, lax.rem(device, 2)
        return z * (1 - y) + (sp - 1 - z) * y

    def device_at(place):
        up = place // (sp // 2)
        return 2 * (place * (1 - up) + (sp - 1 - place) * up) + up

    here = place(s)
    after, before = device_at(lax.rem(here + 1, sp)), device_at(lax.rem(here + sp - 1, sp))
    following, leading = lax.rem(s + 1, sp), lax.rem(s + sp - 1, sp)

    def columns(device):
        return pl.ds(pl.multiple_of(device * chan_dev, chan_dev), chan_dev)

    def ring_view(layer, side, piece, source):
        if side == 0:
            part = model_dev // 2
            return win.at[layer, pl.ds(pl.multiple_of(piece * part, part), part), columns(source)]
        part = row_dev // 2
        return wout.at[layer, pl.ds(pl.multiple_of(source * row_dev + piece * part, part), part)]

    def ring_copy(layer, side, way, turn, back):
        hop = turn // 2 + back
        piece = lax.rem(turn + way, 2)
        origin = here - hop + sp if way == 0 else here + hop
        view = ring_view(layer, side, piece, device_at(lax.rem(origin, sp)))
        return pltpu.make_async_remote_copy(
            src_ref=view, dst_ref=view,
            send_sem=ring_s.at[way, turn], recv_sem=ring_r.at[way, turn],
            device_id={"sp": after if way == 0 else before}, device_id_type=MESH)

    turns = sp - 1
    items = 2 * layers

    def arrive(index):
        item, turn = index // turns, lax.rem(index, turns)
        layer, side = item // 2, lax.rem(item, 2)
        for which in range(2):
            @pl.when(side == which)
            def _():
                for way in range(2):
                    ring_copy(layer, which, way, turn, 1).wait_recv()

                @pl.when((turn < turns - 2) & (item > 0))
                def _():
                    for way in range(2):
                        ring_copy(layer + which - 1, 1 - which, way, turn + 2, 0).wait_send()

                @pl.when(turn < turns - 2)
                def _():
                    for way in range(2):
                        ring_copy(layer, which, way, turn + 2, 0).start()

                @pl.when((turn >= turns - 3) & (turn < turns - 1) & (item + 1 < items))
                def _():
                    for way in range(2):
                        ring_copy(layer, which, way, turn - (turns - 3), 0).wait_send()
                        ring_copy(layer + which, 1 - which, way, turn - (turns - 3), 0).start()

    def at(i):
        return pl.ds(pl.multiple_of(i * rows, rows), rows)

    def load_x(i):
        return pltpu.make_async_copy(x_hbm.at[at(i)], h.at[at(i)], xs.at[i])

    def load_w(layer, side):
        if side == 0:
            return pltpu.make_async_copy(win_hbm.at[layer], win.at[layer, :, columns(s)], ws.at[layer, side])
        return pltpu.make_async_copy(
            wout_hbm.at[layer], wout.at[layer, pl.ds(pl.multiple_of(s * row_dev, row_dev), row_dev)], ws.at[layer, side])

    load_w(0, 0).start()
    for i in range(CHUNKS):
        load_x(last - i).start()
    for layer in range(layers):
        for side in range(2):
            if layer + side > 0:
                load_w(layer, side).start()

    barrier = pltpu.get_barrier_semaphore()
    peers = ({"tp": partner}, {"tp": across}, {"tp": diagonal},
             {"sp": after}, {"sp": before}, {"sp": following}, {"sp": leading})
    for peer in peers:
        pl.semaphore_signal(barrier, inc=1, device_id=peer, device_id_type=MESH)
    own_gain = gains_ref[:, pl.ds(pl.multiple_of(t * model_dev, model_dev), model_dev)].astype(F32)
    for layer in range(layers):
        gain_ref[layer] = own_gain[layer:layer + 1]
    for lg in range(own_groups):
        own_pgain = pgains_ref[:, columns(lg + own_groups * lax.rem(lg + core, 2))].astype(F32)
        for layer in range(layers):
            pgain_ref[layer, :, lg * group:(lg + 1) * group] = own_pgain[layer:layer + 1]
    load_w(0, 0).wait()
    pl.semaphore_wait(barrier, len(peers))
    for turn in range(2):
        for way in range(2):
            ring_copy(0, 0, way, turn, 0).start()
    reach = 2 * HALO
    label_copy = pltpu.make_async_remote_copy(
        src_ref=labels.at[pl.ds(tokens, reach)], dst_ref=before_labels, send_sem=ls, recv_sem=lr,
        device_id={"sp": following}, device_id_type=MESH)

    def distances(ext):
        run = (pltpu.roll(ext, 1, 0) == ext).astype(F32)
        size = 1
        while size < HALO:
            run = run + jnp.where(run == float(size), pltpu.roll(run, size, 0), 0.0)
            size *= 2
        return run[HALO:]

    def prepare():
        for layer in range(layers):
            for side in range(2):
                if layer + side > 0:
                    load_w(layer, side).wait()
        documents = doc_ref[...].astype(F32)
        for j in range(tokens // 128):
            labels[pl.ds(reach + j * 128, 128)] = jnp.broadcast_to(documents[j:j + 1], (128, 128)).T
        label_copy.start()

    def measure():
        label_copy.wait()
        labels[pl.ds(0, reach)] = jnp.where(s == 0, -1.0, before_labels[...])
        pos_ref[pl.ds(0, HALO)] = distances(labels[pl.ds(0, reach)])

        @pl.loop(0, CHUNKS)
        def _(i):
            pos = distances(labels[pl.ds(pl.multiple_of(HALO + i * rows, HALO), rows + HALO)])
            pos_ref[pl.ds(pl.multiple_of(HALO + i * rows, HALO), rows)] = pos
            for w in range(4):
                inverse[w, at(i)] = 1.0 / jnp.minimum(pos + 1.0, float(2 ** (1 + w)))

    def copy_sq(layer, i):
        par = lax.rem(layer, 2)
        return [pltpu.make_async_remote_copy(
            src_ref=sq_own.at[i], dst_ref=sq_in.at[par, i, j], send_sem=sqs.at[i], recv_sem=sqr.at[par, i],
            device_id={"tp": peer}, device_id_type=MESH)
            for j, peer in enumerate((partner, across, diagonal))]

    def copy1(i, lg):
        return pltpu.make_async_remote_copy(
            src_ref=send1.at[lg, i], dst_ref=recv1.at[lg, i], send_sem=s1.at[i], recv_sem=r1.at[lg, i],
            device_id={"tp": partner}, device_id_type=MESH)

    def copy2(layer, i, lg):
        par = lax.rem(layer, 2)
        return pltpu.make_async_remote_copy(
            src_ref=sum2.at[lg, i], dst_ref=recv2.at[par, lg, i], send_sem=s2.at[i], recv_sem=r2.at[par, lg, i],
            device_id={"tp": across}, device_id_type=MESH)

    def copy_part(lg, part):
        par = (layers - 1) % 2
        cut = pl.ds(part * (rows // 2), rows // 2)
        return pltpu.make_async_remote_copy(
            src_ref=sum2.at[lg, 0, cut], dst_ref=recv2.at[par, lg, 0, cut],
            send_sem=s2.at[0], recv_sem=r2.at[par, lg, 0] if part else rh.at[lg],
            device_id={"tp": across}, device_id_type=MESH)

    def normalise_part(lg, part):
        par = (layers - 1) % 2
        cut = pl.ds(part * (rows // 2), rows // 2)
        copy_part(lg, part).wait_recv()
        summed = sum2[lg, 0, cut].astype(F32) + recv2[par, lg, 0, cut].astype(F32)
        zbuf[lg, pl.ds(HALO + part * (rows // 2), rows // 2)] = (summed * scale_ref[0, cut]).astype(BF16)

    def copy3(i, side, lg):
        view = mixed.at[i, :, columns(group_at(side, lg))]
        return pltpu.make_async_remote_copy(
            src_ref=view, dst_ref=view, send_sem=s3.at[i], recv_sem=r3.at[i],
            device_id={"tp": partner}, device_id_type=MESH)

    def halo_copy(layer, lg):
        return pltpu.make_async_remote_copy(
            src_ref=zbuf.at[lg, pl.ds(tokens, HALO)], dst_ref=hrecv.at[layer, lg],
            send_sem=hs.at[layer], recv_sem=hr.at[layer],
            device_id={"sp": following}, device_id_type=MESH)

    def group_at(side, lg):
        return lg + own_groups * lax.rem(lg + side, 2)

    def columns_of(layer, side):
        return jnp.concatenate([win[layer, :, columns(group_at(side, lg))] for lg in range(own_groups)], axis=1)

    def groups_of(distance):
        return (device_at(lax.rem(here - distance + sp, sp)), device_at(lax.rem(here + distance, sp)))

    def owned(g):
        return lax.rem(g // own_groups + g, 2) == core

    def local(g):
        return lax.rem(g, own_groups)

    def gained_of(layer, i):
        wide = h[at(i)].astype(F32)
        squares = wide * wide
        lanes = squares[:, :128]
        for j in range(1, model_dev // 128):
            lanes = lanes + squares[:, j * 128:(j + 1) * 128]
        sq_own[i] = jnp.sum(lanes.T, axis=0, keepdims=True)
        gained = (wide * gain_ref[layer]).astype(BF16)
        for c in copy_sq(layer, i):
            c.start()
        return gained

    def deliver(i, g, value):
        several = value.shape[0] // rows

        @pl.when(owned(g))
        def _():
            for k in range(several):
                own1[local(g), i + k] = value[k * rows:(k + 1) * rows]

        @pl.when(jnp.logical_not(owned(g)))
        def _():
            for k in reversed(range(several)):
                send1[local(g), i + k] = value[k * rows:(k + 1) * rows]
                copy1(i + k, local(g)).start()

    def project_groups(layer, distance, i, several):
        low, high = groups_of(distance)
        span = pl.ds(pl.multiple_of(i * rows, rows), several * rows)

        @pl.when(lax.rem(distance, sp // 2) == 0)
        def _():
            part = jnp.dot(gbuf[span], win[layer, :, columns(low)], preferred_element_type=F32).astype(BF16)
            deliver(i, low, part)

        @pl.when(lax.rem(distance, sp // 2) > 0)
        def _():
            weights = jnp.concatenate([win[layer, :, columns(low)], win[layer, :, columns(high)]], axis=1)
            part = jnp.dot(gbuf[span], weights, preferred_element_type=F32).astype(BF16)
            deliver(i, low, part[:, :group])
            deliver(i, high, part[:, group:])

    def project(layer, i):
        @pl.when(layer > 0)
        def _():
            gbuf[at(i)] = gained_of(layer, i)

        gained = gbuf[at(i)]
        part = jnp.dot(gained, columns_of(layer, 1 - core), preferred_element_type=F32).astype(BF16)
        for lg in range(own_groups):
            @pl.when((layer > 0) | (group_at(1 - core, lg) != s))
            def _():
                send1[lg, i] = part[:, lg * group:(lg + 1) * group]
                copy1(i, lg).start()
        part = jnp.dot(gained, columns_of(layer, core), preferred_element_type=F32).astype(BF16)
        for lg in range(own_groups):
            own1[lg, i] = part[:, lg * group:(lg + 1) * group]

    def add_up(layer, i, lg):
        sum2[lg, i] = (own1[lg, i].astype(F32) + recv1[lg, i].astype(F32)).astype(BF16)

        @pl.when((layer < layers - 1) | (i > 0))
        def _():
            copy2(layer, i, lg).start()

    def each_group(distance, act):
        low, high = groups_of(distance)
        act(low)

        @pl.when(lax.rem(distance, sp // 2) > 0)
        def _():
            act(high)

    def join_groups(layer, distance, i):
        def act(g):
            @pl.when(owned(g))
            def _():
                copy1(i, local(g)).wait_recv()
                add_up(layer, i, local(g))

        each_group(distance, act)

    def join(layer, i):
        for lg in range(own_groups):
            @pl.when((layer > 0) | (group_at(core, lg) != s))
            def _():
                copy1(i, lg).wait_recv()
                add_up(layer, i, lg)

        @pl.when((layer == layers - 1) & (i == 0))
        def _():
            for part in (1, 0):
                for lg in range(own_groups):
                    copy_part(lg, part).start()

    def rescale(layer, i):
        par = lax.rem(layer, 2)
        pltpu.make_async_remote_copy(
            src_ref=sq_in.at[par, i], dst_ref=sq_in.at[par, i], send_sem=sqs.at[i], recv_sem=sqr.at[par, i],
            device_id={"tp": partner}, device_id_type=MESH).wait()
        total = sq_own[i]
        for j in range(3):
            total = total + sq_in[par, i, j]
        scale_ref[i] = jnp.broadcast_to(lax.rsqrt(total / model + EPSILON), (128, rows)).T

    def normalise(layer, i, lg):
        par = lax.rem(layer, 2)
        copy2(layer, i, lg).wait_recv()
        summed = sum2[lg, i].astype(F32) + recv2[par, lg, i].astype(F32)
        zbuf[lg, pl.ds(pl.multiple_of(HALO + i * rows, HALO), rows)] = (summed * scale_ref[i]).astype(BF16)

    def pool(layer, i, lg):
        wide_at = pl.ds(pl.multiple_of(i * rows, HALO), rows + HALO)
        pos = pos_ref[wide_at]
        z = zbuf[lg, wide_at].astype(F32)
        window = 2 ** (1 + lg % 4)
        total = z
        size = 1
        while size < window:
            total = total + jnp.where(pos >= size, pltpu.roll(total, size, 0), 0.0)
            size *= 2
        pooled = (total[HALO:] * inverse[lg % 4, at(i)] - z[HALO:]).astype(BF16)
        blended = jnp.dot(pooled, mix_ref[layer, group_at(core, lg)], preferred_element_type=F32)
        mixed[i, :, columns(group_at(core, lg))] = (blended * pgain_ref[layer, :, lg * group:(lg + 1) * group]).astype(BF16)
        copy3(i, core, lg).start()

    def side_of(i, side):
        return mixed.at[i, :, pl.ds(pl.multiple_of(side * half, half), half)]

    def take_halo(layer):
        pltpu.make_async_remote_copy(
            src_ref=zbuf.at[:, pl.ds(tokens, HALO)], dst_ref=hrecv.at[layer], send_sem=hs.at[layer], recv_sem=hr.at[layer],
            device_id={"sp": following}, device_id_type=MESH).wait()
        zbuf[:, pl.ds(0, HALO)] = hrecv[layer]

    def finish(layer, i):
        for src, dst, sems in ((send1.at[:, i], recv1.at[:, i], s1), (sum2.at[:, i], recv2.at[0, :, i], s2),
                               (side_of(i, core), side_of(i, core), s3)):
            pltpu.make_async_remote_copy(
                src_ref=src, dst_ref=dst, send_sem=sems.at[i], recv_sem=r3.at[i],
                device_id={"tp": partner}, device_id_type=MESH).wait_send()
        pltpu.make_async_remote_copy(
            src_ref=side_of(i, 1 - core), dst_ref=side_of(i, 1 - core), send_sem=s3.at[i], recv_sem=r3.at[i],
            device_id={"tp": partner}, device_id_type=MESH).wait_recv()
        for j in range(2):
            cols = slice(j * (model_dev // 2), (j + 1) * (model_dev // 2))
            update = jnp.dot(mixed[i], wout[layer, :, cols], preferred_element_type=F32)
            h[at(i), cols] = (h[at(i), cols].astype(F32) + update).astype(BF16)


    spans = sp // 2 + 1

    @pl.loop(0, layers + 1)
    def _(layer):
        edge = EDGE + layer
        ending = layer // layers
        live = layer < layers
        slots = (spans + edge) * (1 - ending) + ending

        @pl.loop(0, slots)
        def _(q):
            def past(k):
                return (q + 15 - k) // 16

            middle, final = lax.rem(layer, 2), layer // 2
            turn = 2 * q + middle * (14 - past(4)) + final * (28 - past(3) - past(4) - past(7))
            opening = (q == 0) & (layer > 0)
            single = opening | ((middle == 1) & (q == 4)) | ((final == 1) & ((q == 3) | (q == 4) | (q == 7)))
            everything = ((q == 0) & (layer == 0)).astype(jnp.int32)
            count = CHUNKS - edge + edge * everything

            inline = ((q == 0) | ((q == 1) & (layer == 0))).astype(jnp.int32)

            def gain(i):
                @pl.when(layer == 0)
                def _():
                    load_x(i).wait()

                @pl.when(layer == 1)
                def _():
                    finish(layer - 1, i)

                gbuf[at(i)] = gained_of(layer, i)

            @pl.when(live & (q < spans))
            def _():
                @pl.loop(0, count // 2)
                def _(j):
                    @pl.when(q == 0)
                    def _():
                        @pl.loop(0, 2)
                        def _(k):
                            gain(last - 2 * j - k)

                    project_groups(layer, q, last - 2 * j - 1, 2)

                    early = opening & (final == 1) & (j == 0)

                    @pl.when(early)
                    def _():
                        @pl.loop(0, 2)
                        def _(k):
                            finish(layer - 1, last - 2 - k)

                    @pl.when(early | ((inline == 1) & (j > 0) & ((final == 0) | (q > 0))))
                    def _():
                        for k in range(2):
                            join_groups(layer, q, last - 2 * j + 2 - 2 * early.astype(jnp.int32) - k)

                    @pl.when(opening & (((middle == 1) & (j == 0)) | (j == 1)))
                    def _():
                        arrive(turn + j)

                @pl.when(lax.rem(count, 2) == 1)
                def _():
                    @pl.when(q == 0)
                    def _():
                        gain(CHUNKS - count)

                    project_groups(layer, q, CHUNKS - count, 1)

            @pl.when(q >= spans)
            def _():
                project(layer, edge - 1 - (q - spans))

            one = (layer > 0) & (((ending == 1) & (q < 2)) | (live & (q > 0) & (q < 5) & (q + edge > 4)))

            @pl.when(one)
            def _():
                finish(layer - 1, 4 - ending - q)

            @pl.when(live & (q < spans))
            def _():
                joined = (count // 2 - 1) * 2 * inline

                @pl.loop(joined, count)
                def _(j):
                    join_groups(layer, q, last - j)

            @pl.when(q >= spans)
            def _():
                join(layer, edge - 1 - (q - spans))

            @pl.when(live & (turn < turns * items) & jnp.logical_not(opening))
            def _():
                arrive(turn)

            @pl.when((layer > 0) & live & (q == slots - 1))
            def _():
                @pl.loop(0, 2 + 2 * final)
                def _(j):
                    finish(layer, last - j)

            more = live & (turn + 1 < turns * items) & jnp.logical_not(single)
            lag = 3 - (layer + 9) // 10
            reps = 1 + ((layer == 0) & (q == slots - 1)).astype(jnp.int32)

            @pl.when((layer == 0) & (q == 0))
            def _():
                prepare()

            @pl.when((layer == 0) & (q == 1))
            def _():
                measure()

            old = (layer > 0) & (((ending == 1) & (q < 2)) | (live & (q == 1)))

            @pl.when(old | (q >= spans + 2))
            def _():
                fresh = q // (spans + 2)
                of = layer - 1 + fresh
                first = (1 - q * ending) * (1 - fresh) + (edge - 1 - (q - 2 - spans)) * fresh

                @pl.loop(0, 1 + (1 - fresh) * (1 - ending))
                def _(j):
                    i = first - j
                    rescale(of, i)

                    @pl.when(i == 0)
                    def _():
                        take_halo(of)

                    for lg in range(own_groups):
                        normalise(of, i, lg)
                        pool(of, i + 1, lg)

                        @pl.when(i == 0)
                        def _():
                            pool(of, i, lg)

            @pl.loop(0, reps)
            def _(rep):
                @pl.when(live & (q >= lag) & (q < spans + lag))
                def _():
                    distance = q - lag + rep

                    @pl.loop(0, CHUNKS - edge)
                    def _(j):
                        @pl.when(distance == 0)
                        def _():
                            rescale(layer, last - j)

                        def act(g):
                            @pl.when(owned(g))
                            def _():
                                normalise(layer, last - j, local(g))

                                @pl.when(j == 0)
                                def _():
                                    halo_copy(layer, local(g)).start()
                        each_group(distance, act)

                    @pl.loop(0, CHUNKS - edge - 1)
                    def _(j):
                        def act(g):
                            for lg in range(own_groups):
                                @pl.when(owned(g) & (local(g) == lg))
                                def _():
                                    pool(layer, last - j, lg)
                        each_group(distance, act)

                @pl.when(more & (rep == reps - 1))
                def _():
                    arrive(turn + 1)

    rescale(layers - 1, 0)
    take_halo(layers - 1)
    for i in (1, 0):
        for lg in range(own_groups):
            normalise_part(lg, i)
            pool(layers - 1, i, lg)

        @pl.loop(0, 2 - i)
        def _(j):
            finish(layers - 1, 1 + i - j)

    for way in range(2):
        for turn in range(turns):
            ring_copy(layers - 1, 1, way, turn, 0).wait_send()


def body(sp, tp, stream, doc_ids, norm_gain, proj_in, mix_pool, pool_gain, proj_out):
    layers, model_dev, chan_dev = proj_in.shape
    tokens = stream.shape[0]
    rows = tokens // CHUNKS
    channels = chan_dev * sp
    half = channels // 2
    group = mix_pool.shape[-1]
    own = half // group
    dma, vmem = pltpu.SemaphoreType.DMA, pltpu.VMEM
    local, remote = pl.BlockSpec(memory_space=pltpu.VMEM), pl.BlockSpec(memory_space=pl.ANY)
    return pl.pallas_call(
        functools.partial(mixer, sp, tp),
        out_shape=pltpu.VMEM(stream.shape, BF16),
        in_specs=[remote, local, local, remote, local, local, remote],
        out_specs=local,
        scratch_shapes=[
            vmem((layers, model_dev, channels), BF16),
            vmem((layers, channels, model_dev), BF16),
            vmem((tokens, model_dev), BF16),
            vmem((own, CHUNKS, rows, group), BF16),
            vmem((own, CHUNKS, rows, group), BF16),
            vmem((own, CHUNKS, rows, group), BF16),
            vmem((own, CHUNKS, rows, group), BF16),
            vmem((2, own, CHUNKS, rows, group), BF16),
            vmem((CHUNKS, rows, channels), BF16),
            vmem((own, HALO + tokens, group), BF16),
            vmem((layers, own, HALO, group), BF16),
            vmem((CHUNKS, 1, rows), F32),
            vmem((2, CHUNKS, 3, 1, rows), F32),
            vmem((CHUNKS, rows, 128), F32),
            vmem((2 * HALO + tokens, 128), F32),
            vmem((2 * HALO, 128), F32),
            vmem((HALO + tokens, 128), F32),
            vmem((4, tokens, 128), F32),
            vmem((layers, 1, model_dev), F32),
            vmem((layers, 1, half), F32),
            dma((CHUNKS,)), dma((layers, 2)),
            dma, dma,
            dma((2, sp - 1)), dma((2, sp - 1)),
            dma((CHUNKS,)), dma((2, CHUNKS)),
            dma((CHUNKS,)), dma((own, CHUNKS)),
            dma((CHUNKS,)), dma((2, own, CHUNKS)), dma((own,)),
            dma((CHUNKS,)), dma((CHUNKS,)),
            dma((layers,)), dma((layers,)),
        ],
        compiler_params=pltpu.CompilerParams(
            collective_id=0, has_side_effects=True, vmem_limit_bytes=56 * 2**20),
    )(stream, doc_ids.reshape(-1, 128), norm_gain, proj_in, mix_pool, pool_gain, proj_out)


span_reach = 15


def shifted(value, axis, steps):
    count = lax.axis_size(axis)
    initial, last = (max(0, -steps), min(count, count - steps))
    return lax.ppermute(value, axis, [(source, source + steps) for source in range(initial, last)])


def span_pool(padded, labels, widths):
    kept = padded.shape[0] - span_reach
    own_label = labels[span_reach:]
    summed = jnp.zeros((kept, padded.shape[1]), jnp.float32)
    counted = jnp.zeros((kept, padded.shape[1]), jnp.float32)
    for offset in range(span_reach + 1):
        first = span_reach - offset
        member = (labels[first : first + kept] == own_label)[:, None] & (offset < widths)[None, :]
        factor = member.astype(jnp.float32)
        summed = summed + padded[first : first + kept] * factor
        counted = counted + factor
    return summed / counted - padded[span_reach:]


def plain_body(stream, doc_ids, norm_gain, proj_in, mix_pool, pool_gain, proj_out):
    width_dev = stream.shape[1]
    tp_count = lax.axis_size("tp")
    model_width = width_dev * tp_count
    group_size = mix_pool.shape[2]
    channels = proj_in.shape[2] * lax.axis_size("sp")
    local = channels // tp_count
    groups_dev = local // group_size
    column = lax.axis_index("tp")
    chan_ids = column * local + jnp.arange(local, dtype=jnp.int32)
    widths = jnp.left_shift(jnp.int32(2), chan_ids // group_size % 4)
    labels = (doc_ids + 1).astype(jnp.bfloat16)
    hidden_state = stream
    layer_count = proj_in.shape[0]
    in_whole, out_whole = (
        lax.all_gather(proj_in, "sp", axis=2, tiled=True),
        lax.all_gather(proj_out, "sp", axis=1, tiled=True),
    )
    for layer in range(layer_count):
        row_count = hidden_state.shape[0]
        wide = hidden_state.astype(jnp.float32)
        own_squares = jnp.sum(wide * wide, axis=1)
        gain = lax.dynamic_slice_in_dim(norm_gain[layer], column * width_dev, width_dev).astype(
            jnp.float32
        )
        gained = (wide * gain[None, :]).astype(jnp.bfloat16)
        partial_value = jnp.dot(gained, in_whole[layer], preferred_element_type=jnp.float32)
        squares = lax.psum(own_squares, "tp")
        summed_in = lax.psum_scatter(
            partial_value.astype(jnp.bfloat16), "tp", scatter_dimension=1, tiled=True
        ).astype(jnp.float32)
        row_scale = lax.rsqrt(squares / model_width + EPSILON)
        mixed_in = (summed_in * row_scale[:, None]).astype(jnp.bfloat16)
        before, before_labels = shifted((mixed_in[-span_reach:], labels[-span_reach:]), "sp", 1)
        padded = jnp.concatenate([before, mixed_in], axis=0).astype(jnp.float32)
        tags = jnp.concatenate([before_labels, labels], axis=0)
        pooled = span_pool(padded, tags, widths).astype(jnp.bfloat16)
        grouped = pooled.reshape(row_count, groups_dev, group_size)
        mixing = lax.dynamic_slice_in_dim(mix_pool[layer], column * groups_dev, groups_dev, 0)
        blended = jnp.einsum(
            "tgc,gcd->tgd", grouped, mixing, preferred_element_type=jnp.float32
        ).reshape(row_count, local)
        scale = lax.dynamic_slice_in_dim(pool_gain[layer], column * local, local).astype(
            jnp.float32
        )
        mixed = (blended * scale[None, :]).astype(jnp.bfloat16)
        full_mixed = lax.all_gather(mixed, "tp", axis=1, tiled=True)
        update = jnp.dot(full_mixed, out_whole[layer], preferred_element_type=jnp.float32)
        hidden_state = (wide + update).astype(jnp.bfloat16)
    return hidden_state


def solution(mesh):
    sp, tp = mesh.shape["sp"], mesh.shape["tp"]
    in_specs = (P("sp", "tp"), P("sp"), P(), P(None, "tp", "sp"), P(), P(), P(None, "sp", "tp"))

    def whole(stream, doc_ids, norm_gain, proj_in, mix_pool, pool_gain, proj_out):
        layers, _, channels = proj_in.shape
        group = mix_pool.shape[2]
        fits = (tp == 4 and sp == RING and layers == LAYERS and channels == sp * group and group == 128
                and mix_pool.shape[1] % 8 == 0 and stream.shape[0] % (sp * CHUNKS * 128) == 0)
        part = functools.partial(body, sp, tp) if fits else plain_body
        return jax.shard_map(part, mesh=mesh, in_specs=in_specs, out_specs=P("sp", "tp"), check_vma=False)(
            stream, doc_ids, norm_gain, proj_in, mix_pool, pool_gain, proj_out)

    return whole
```

```python
import functools

import jax
import jax.numpy as jnp
from jax import lax
from jax.experimental import pallas as pl
from jax.experimental.pallas import tpu as pltpu
from jax.sharding import PartitionSpec as P

EPSILON = 1e-06
HALO = 16
CHUNKS = 8
EDGE = 2
RING = 8
LAYERS = 3
MESH = pl.DeviceIdType.MESH
F32, BF16 = jnp.float32, jnp.bfloat16


def mixer(sp, tp, x_hbm, doc_ref, gains_ref, win_hbm, mix_ref, pgains_ref, wout_hbm, h,
          win, wout, gbuf, send1, own1, recv1, sum2, recv2, mixed, zbuf, hrecv,
          sq_own, sq_in, scale_ref, labels, before_labels, pos_ref, inverse, gain_ref, pgain_ref,
          xs, ws, ls, lr, ring_s, ring_r, sqs, sqr, s1, r1, s2, r2, rh, s3, r3, hs, hr):
    layers, model_dev, chan_dev = win_hbm.shape
    tokens = h.shape[0]
    rows = tokens // CHUNKS
    channels = chan_dev * sp
    half = channels // 2
    group = mix_ref.shape[-1]
    own_groups = half // group
    model = model_dev * tp
    row_dev = wout_hbm.shape[1]
    last = CHUNKS - 1
    s, t = lax.axis_index("sp"), lax.axis_index("tp")
    core = lax.rem(t, 2)
    partner = t + 1 - 2 * core
    across = lax.rem(t + 2, tp)
    diagonal = lax.rem(partner + 2, tp)

    def place(device):
        z, y = device // 2, lax.rem(device, 2)
        return z * (1 - y) + (sp - 1 - z) * y

    def device_at(place):
        up = place // (sp // 2)
        return 2 * (place * (1 - up) + (sp - 1 - place) * up) + up

    here = place(s)
    after, before = device_at(lax.rem(here + 1, sp)), device_at(lax.rem(here + sp - 1, sp))
    following, leading = lax.rem(s + 1, sp), lax.rem(s + sp - 1, sp)

    def columns(device):
        return pl.ds(pl.multiple_of(device * chan_dev, chan_dev), chan_dev)

    def ring_view(layer, side, piece, source):
        if side == 0:
            part = model_dev // 2
            return win.at[layer, pl.ds(pl.multiple_of(piece * part, part), part), columns(source)]
        part = row_dev // 2
        return wout.at[layer, pl.ds(pl.multiple_of(source * row_dev + piece * part, part), part)]

    def ring_copy(layer, side, way, turn, back):
        hop = turn // 2 + back
        piece = lax.rem(turn + way, 2)
        origin = here - hop + sp if way == 0 else here + hop
        view = ring_view(layer, side, piece, device_at(lax.rem(origin, sp)))
        return pltpu.make_async_remote_copy(
            src_ref=view, dst_ref=view,
            send_sem=ring_s.at[way, turn], recv_sem=ring_r.at[way, turn],
            device_id={"sp": after if way == 0 else before}, device_id_type=MESH)

    turns = sp - 1
    items = 2 * layers

    def arrive(index):
        item, turn = index // turns, lax.rem(index, turns)
        layer, side = item // 2, lax.rem(item, 2)
        for which in range(2):
            @pl.when(side == which)
            def _():
                for way in range(2):
                    ring_copy(layer, which, way, turn, 1).wait_recv()

                @pl.when((turn < turns - 2) & (item > 0))
                def _():
                    for way in range(2):
                        ring_copy(layer + which - 1, 1 - which, way, turn + 2, 0).wait_send()

                @pl.when(turn < turns - 2)
                def _():
                    for way in range(2):
                        ring_copy(layer, which, way, turn + 2, 0).start()

                @pl.when((turn >= turns - 3) & (turn < turns - 1) & (item + 1 < items))
                def _():
                    for way in range(2):
                        ring_copy(layer, which, way, turn - (turns - 3), 0).wait_send()
                        ring_copy(layer + which, 1 - which, way, turn - (turns - 3), 0).start()

    def at(i):
        return pl.ds(pl.multiple_of(i * rows, rows), rows)

    def load_x(i):
        return pltpu.make_async_copy(x_hbm.at[at(i)], h.at[at(i)], xs.at[i])

    def load_w(layer, side):
        if side == 0:
            return pltpu.make_async_copy(win_hbm.at[layer], win.at[layer, :, columns(s)], ws.at[layer, side])
        return pltpu.make_async_copy(
            wout_hbm.at[layer], wout.at[layer, pl.ds(pl.multiple_of(s * row_dev, row_dev), row_dev)], ws.at[layer, side])

    load_w(0, 0).start()
    for i in range(CHUNKS):
        load_x(last - i).start()
    for layer in range(layers):
        for side in range(2):
            if layer + side > 0:
                load_w(layer, side).start()

    barrier = pltpu.get_barrier_semaphore()
    peers = ({"tp": partner}, {"tp": across}, {"tp": diagonal},
             {"sp": after}, {"sp": before}, {"sp": following}, {"sp": leading})
    for peer in peers:
        pl.semaphore_signal(barrier, inc=1, device_id=peer, device_id_type=MESH)
    own_gain = gains_ref[:, pl.ds(pl.multiple_of(t * model_dev, model_dev), model_dev)].astype(F32)
    for layer in range(layers):
        gain_ref[layer] = own_gain[layer:layer + 1]
    for lg in range(own_groups):
        own_pgain = pgains_ref[:, columns(lg + own_groups * lax.rem(lg + core, 2))].astype(F32)
        for layer in range(layers):
            pgain_ref[layer, :, lg * group:(lg + 1) * group] = own_pgain[layer:layer + 1]
    load_w(0, 0).wait()
    pl.semaphore_wait(barrier, len(peers))
    for turn in range(2):
        for way in range(2):
            ring_copy(0, 0, way, turn, 0).start()
    reach = 2 * HALO
    label_copy = pltpu.make_async_remote_copy(
        src_ref=labels.at[pl.ds(tokens, reach)], dst_ref=before_labels, send_sem=ls, recv_sem=lr,
        device_id={"sp": following}, device_id_type=MESH)

    def distances(ext):
        run = (pltpu.roll(ext, 1, 0) == ext).astype(F32)
        size = 1
        while size < HALO:
            run = run + jnp.where(run == float(size), pltpu.roll(run, size, 0), 0.0)
            size *= 2
        return run[HALO:]

    def prepare():
        for layer in range(layers):
            for side in range(2):
                if layer + side > 0:
                    load_w(layer, side).wait()
        documents = doc_ref[...].astype(F32)
        for j in range(tokens // 128):
            labels[pl.ds(reach + j * 128, 128)] = jnp.broadcast_to(documents[j:j + 1], (128, 128)).T
        label_copy.start()

    def measure():
        label_copy.wait()
        labels[pl.ds(0, reach)] = jnp.where(s == 0, -1.0, before_labels[...])
        pos_ref[pl.ds(0, HALO)] = distances(labels[pl.ds(0, reach)])

        @pl.loop(0, CHUNKS)
        def _(i):
            pos = distances(labels[pl.ds(pl.multiple_of(HALO + i * rows, HALO), rows + HALO)])
            pos_ref[pl.ds(pl.multiple_of(HALO + i * rows, HALO), rows)] = pos
            for w in range(4):
                inverse[w, at(i)] = 1.0 / jnp.minimum(pos + 1.0, float(2 ** (1 + w)))

    def copy_sq(layer, i):
        par = lax.rem(layer, 2)
        return [pltpu.make_async_remote_copy(
            src_ref=sq_own.at[i], dst_ref=sq_in.at[par, i, j], send_sem=sqs.at[i], recv_sem=sqr.at[par, i],
            device_id={"tp": peer}, device_id_type=MESH)
            for j, peer in enumerate((partner, across, diagonal))]

    def copy1(i, lg):
        return pltpu.make_async_remote_copy(
            src_ref=send1.at[lg, i], dst_ref=recv1.at[lg, i], send_sem=s1.at[i], recv_sem=r1.at[lg, i],
            device_id={"tp": partner}, device_id_type=MESH)

    def copy2(layer, i, lg):
        par = lax.rem(layer, 2)
        return pltpu.make_async_remote_copy(
            src_ref=sum2.at[lg, i], dst_ref=recv2.at[par, lg, i], send_sem=s2.at[i], recv_sem=r2.at[par, lg, i],
            device_id={"tp": across}, device_id_type=MESH)

    def copy_part(lg, part):
        par = (layers - 1) % 2
        cut = pl.ds(part * (rows // 2), rows // 2)
        return pltpu.make_async_remote_copy(
            src_ref=sum2.at[lg, 0, cut], dst_ref=recv2.at[par, lg, 0, cut],
            send_sem=s2.at[0], recv_sem=r2.at[par, lg, 0] if part else rh.at[lg],
            device_id={"tp": across}, device_id_type=MESH)

    def normalise_part(lg, part):
        par = (layers - 1) % 2
        cut = pl.ds(part * (rows // 2), rows // 2)
        copy_part(lg, part).wait_recv()
        summed = sum2[lg, 0, cut].astype(F32) + recv2[par, lg, 0, cut].astype(F32)
        zbuf[lg, pl.ds(HALO + part * (rows // 2), rows // 2)] = (summed * scale_ref[0, cut]).astype(BF16)

    def copy3(i, side, lg):
        view = mixed.at[i, :, columns(group_at(side, lg))]
        return pltpu.make_async_remote_copy(
            src_ref=view, dst_ref=view, send_sem=s3.at[i], recv_sem=r3.at[i],
            device_id={"tp": partner}, device_id_type=MESH)

    def halo_copy(layer, lg):
        return pltpu.make_async_remote_copy(
            src_ref=zbuf.at[lg, pl.ds(tokens, HALO)], dst_ref=hrecv.at[layer, lg],
            send_sem=hs.at[layer], recv_sem=hr.at[layer],
            device_id={"sp": following}, device_id_type=MESH)

    def group_at(side, lg):
        return lg + own_groups * lax.rem(lg + side, 2)

    def columns_of(layer, side):
        return jnp.concatenate([win[layer, :, columns(group_at(side, lg))] for lg in range(own_groups)], axis=1)

    def groups_of(distance):
        return (device_at(lax.rem(here - distance + sp, sp)), device_at(lax.rem(here + distance, sp)))

    def owned(g):
        return lax.rem(g // own_groups + g, 2) == core

    def local(g):
        return lax.rem(g, own_groups)

    def gained_of(layer, i):
        wide = h[at(i)].astype(F32)
        squares = wide * wide
        lanes = squares[:, :128]
        for j in range(1, model_dev // 128):
            lanes = lanes + squares[:, j * 128:(j + 1) * 128]
        sq_own[i] = jnp.sum(lanes.T, axis=0, keepdims=True)
        gained = (wide * gain_ref[layer]).astype(BF16)
        for c in copy_sq(layer, i):
            c.start()
        return gained

    def deliver(i, g, value):
        several = value.shape[0] // rows

        @pl.when(owned(g))
        def _():
            for k in range(several):
                own1[local(g), i + k] = value[k * rows:(k + 1) * rows]

        @pl.when(jnp.logical_not(owned(g)))
        def _():
            for k in reversed(range(several)):
                send1[local(g), i + k] = value[k * rows:(k + 1) * rows]
                copy1(i + k, local(g)).start()

    def project_groups(layer, distance, i, several):
        low, high = groups_of(distance)
        span = pl.ds(pl.multiple_of(i * rows, rows), several * rows)

        @pl.when(lax.rem(distance, sp // 2) == 0)
        def _():
            part = jnp.dot(gbuf[span], win[layer, :, columns(low)], preferred_element_type=F32).astype(BF16)
            deliver(i, low, part)

        @pl.when(lax.rem(distance, sp // 2) > 0)
        def _():
            weights = jnp.concatenate([win[layer, :, columns(low)], win[layer, :, columns(high)]], axis=1)
            part = jnp.dot(gbuf[span], weights, preferred_element_type=F32).astype(BF16)
            deliver(i, low, part[:, :group])
            deliver(i, high, part[:, group:])

    def project(layer, i):
        @pl.when(layer > 0)
        def _():
            gbuf[at(i)] = gained_of(layer, i)

        gained = gbuf[at(i)]
        part = jnp.dot(gained, columns_of(layer, 1 - core), preferred_element_type=F32).astype(BF16)
        for lg in range(own_groups):
            @pl.when((layer > 0) | (group_at(1 - core, lg) != s))
            def _():
                send1[lg, i] = part[:, lg * group:(lg + 1) * group]
                copy1(i, lg).start()
        part = jnp.dot(gained, columns_of(layer, core), preferred_element_type=F32).astype(BF16)
        for lg in range(own_groups):
            own1[lg, i] = part[:, lg * group:(lg + 1) * group]

    def add_up(layer, i, lg):
        sum2[lg, i] = (own1[lg, i].astype(F32) + recv1[lg, i].astype(F32)).astype(BF16)

        @pl.when((layer < layers - 1) | (i > 0))
        def _():
            copy2(layer, i, lg).start()

    def each_group(distance, act):
        low, high = groups_of(distance)
        act(low)

        @pl.when(lax.rem(distance, sp // 2) > 0)
        def _():
            act(high)

    def join_groups(layer, distance, i):
        def act(g):
            @pl.when(owned(g))
            def _():
                copy1(i, local(g)).wait_recv()
                add_up(layer, i, local(g))

        each_group(distance, act)

    def join(layer, i):
        for lg in range(own_groups):
            @pl.when((layer > 0) | (group_at(core, lg) != s))
            def _():
                copy1(i, lg).wait_recv()
                add_up(layer, i, lg)

        @pl.when((layer == layers - 1) & (i == 0))
        def _():
            for part in (1, 0):
                for lg in range(own_groups):
                    copy_part(lg, part).start()

    def rescale(layer, i):
        par = lax.rem(layer, 2)
        pltpu.make_async_remote_copy(
            src_ref=sq_in.at[par, i], dst_ref=sq_in.at[par, i], send_sem=sqs.at[i], recv_sem=sqr.at[par, i],
            device_id={"tp": partner}, device_id_type=MESH).wait()
        total = sq_own[i]
        for j in range(3):
            total = total + sq_in[par, i, j]
        scale_ref[i] = jnp.broadcast_to(lax.rsqrt(total / model + EPSILON), (128, rows)).T

    def normalise(layer, i, lg):
        par = lax.rem(layer, 2)
        copy2(layer, i, lg).wait_recv()
        summed = sum2[lg, i].astype(F32) + recv2[par, lg, i].astype(F32)
        zbuf[lg, pl.ds(pl.multiple_of(HALO + i * rows, HALO), rows)] = (summed * scale_ref[i]).astype(BF16)

    def pool(layer, i, lg):
        wide_at = pl.ds(pl.multiple_of(i * rows, HALO), rows + HALO)
        pos = pos_ref[wide_at]
        z = zbuf[lg, wide_at].astype(F32)
        window = 2 ** (1 + lg % 4)
        total = z
        size = 1
        while size < window:
            total = total + jnp.where(pos >= size, pltpu.roll(total, size, 0), 0.0)
            size *= 2
        pooled = (total[HALO:] * inverse[lg % 4, at(i)] - z[HALO:]).astype(BF16)
        blended = jnp.dot(pooled, mix_ref[layer, group_at(core, lg)], preferred_element_type=F32)
        mixed[i, :, columns(group_at(core, lg))] = (blended * pgain_ref[layer, :, lg * group:(lg + 1) * group]).astype(BF16)
        copy3(i, core, lg).start()

    def side_of(i, side):
        return mixed.at[i, :, pl.ds(pl.multiple_of(side * half, half), half)]

    def take_halo(layer):
        pltpu.make_async_remote_copy(
            src_ref=zbuf.at[:, pl.ds(tokens, HALO)], dst_ref=hrecv.at[layer], send_sem=hs.at[layer], recv_sem=hr.at[layer],
            device_id={"sp": following}, device_id_type=MESH).wait()
        zbuf[:, pl.ds(0, HALO)] = hrecv[layer]

    def finish(layer, i):
        for src, dst, sems in ((send1.at[:, i], recv1.at[:, i], s1), (sum2.at[:, i], recv2.at[0, :, i], s2),
                               (side_of(i, core), side_of(i, core), s3)):
            pltpu.make_async_remote_copy(
                src_ref=src, dst_ref=dst, send_sem=sems.at[i], recv_sem=r3.at[i],
                device_id={"tp": partner}, device_id_type=MESH).wait_send()
        pltpu.make_async_remote_copy(
            src_ref=side_of(i, 1 - core), dst_ref=side_of(i, 1 - core), send_sem=s3.at[i], recv_sem=r3.at[i],
            device_id={"tp": partner}, device_id_type=MESH).wait_recv()
        for j in range(2):
            cols = slice(j * (model_dev // 2), (j + 1) * (model_dev // 2))
            update = jnp.dot(mixed[i], wout[layer, :, cols], preferred_element_type=F32)
            h[at(i), cols] = (h[at(i), cols].astype(F32) + update).astype(BF16)


    spans = sp // 2 + 1

    @pl.loop(0, layers + 1)
    def _(layer):
        edge = EDGE + layer
        ending = layer // layers
        live = layer < layers
        slots = (spans + edge) * (1 - ending) + ending

        @pl.loop(0, slots)
        def _(q):
            def past(k):
                return (q + 15 - k) // 16

            middle, final = lax.rem(layer, 2), layer // 2
            turn = 2 * q + middle * (14 - past(4)) + final * (28 - past(3) - past(4) - past(7))
            opening = (q == 0) & (layer > 0)
            single = opening | ((middle == 1) & (q == 4)) | ((final == 1) & ((q == 3) | (q == 4) | (q == 7)))
            everything = ((q == 0) & (layer == 0)).astype(jnp.int32)
            count = CHUNKS - edge + edge * everything

            inline = ((q == 0) | ((q == 1) & (layer == 0))).astype(jnp.int32)

            def gain(i):
                @pl.when(layer == 0)
                def _():
                    load_x(i).wait()

                @pl.when(layer == 1)
                def _():
                    finish(layer - 1, i)

                gbuf[at(i)] = gained_of(layer, i)

            @pl.when(live & (q < spans))
            def _():
                @pl.loop(0, count // 2)
                def _(j):
                    @pl.when(q == 0)
                    def _():
                        @pl.loop(0, 2)
                        def _(k):
                            gain(last - 2 * j - k)

                    @pl.when((middle == 1) & (q == 0) & (j > 0))
                    def _():
                        for k in range(2):
                            join_groups(layer, q, last - 2 * j + 2 - k)

                    project_groups(layer, q, last - 2 * j - 1, 2)

                    early = opening & (final == 1) & (j == 0)

                    @pl.when(early)
                    def _():
                        @pl.loop(0, 2)
                        def _(k):
                            finish(layer - 1, last - 2 - k)

                    @pl.when(early | ((inline == 1) & (j > 0) & (layer == 0)))
                    def _():
                        for k in range(2):
                            join_groups(layer, q, last - 2 * j + 2 - 2 * early.astype(jnp.int32) - k)

                    @pl.when(opening & (((middle == 1) & (j == 0)) | (j == 1)))
                    def _():
                        arrive(turn + j)

                @pl.when(lax.rem(count, 2) == 1)
                def _():
                    @pl.when(q == 0)
                    def _():
                        gain(CHUNKS - count)

                    project_groups(layer, q, CHUNKS - count, 1)

            @pl.when(q >= spans)
            def _():
                project(layer, edge - 1 - (q - spans))

            @pl.when(live & (q < spans) & (inline == 0))
            def _():
                @pl.loop(0, count - 2)
                def _(j):
                    join_groups(layer, q, last - j)

            one = (layer > 0) & (((ending == 1) & (q < 2)) | (live & (q > 0) & (q < 5) & (q + edge > 4)))

            @pl.when(one)
            def _():
                finish(layer - 1, 4 - ending - q)

            @pl.when(live & (q < spans))
            def _():
                joined = (count // 2 - 1) * 2 * inline + (count - 2) * (1 - inline)

                @pl.loop(joined, count)
                def _(j):
                    join_groups(layer, q, last - j)

            @pl.when(q >= spans)
            def _():
                join(layer, edge - 1 - (q - spans))

            @pl.when(live & (turn < turns * items) & jnp.logical_not(opening))
            def _():
                arrive(turn)

            @pl.when((layer > 0) & live & (q == slots - 1))
            def _():
                @pl.loop(0, 2 + 2 * final)
                def _(j):
                    finish(layer, last - j)

            more = live & (turn + 1 < turns * items) & jnp.logical_not(single)
            lag = 3 - (layer + 9) // 10
            reps = 1 + ((layer == 0) & (q == slots - 1)).astype(jnp.int32)

            @pl.when((layer == 0) & (q == 0))
            def _():
                prepare()

            @pl.when((layer == 0) & (q == 1))
            def _():
                measure()

            old = (layer > 0) & (((ending == 1) & (q < 2)) | (live & (q == 1)))

            @pl.when(old | (q >= spans + 2))
            def _():
                fresh = q // (spans + 2)
                of = layer - 1 + fresh
                first = (1 - q * ending) * (1 - fresh) + (edge - 1 - (q - 2 - spans)) * fresh

                @pl.loop(0, 1 + (1 - fresh) * (1 - ending))
                def _(j):
                    i = first - j
                    rescale(of, i)

                    @pl.when(i == 0)
                    def _():
                        take_halo(of)

                    for lg in range(own_groups):
                        normalise(of, i, lg)
                        pool(of, i + 1, lg)

                        @pl.when(i == 0)
                        def _():
                            pool(of, i, lg)

            @pl.loop(0, reps)
            def _(rep):
                @pl.when(live & (q >= lag) & (q < spans + lag))
                def _():
                    distance = q - lag + rep

                    @pl.loop(0, CHUNKS - edge)
                    def _(j):
                        @pl.when(distance == 0)
                        def _():
                            rescale(layer, last - j)

                        def act(g):
                            @pl.when(owned(g))
                            def _():
                                normalise(layer, last - j, local(g))

                                @pl.when(j == 0)
                                def _():
                                    halo_copy(layer, local(g)).start()
                        each_group(distance, act)

                    @pl.loop(0, CHUNKS - edge - 1)
                    def _(j):
                        def act(g):
                            for lg in range(own_groups):
                                @pl.when(owned(g) & (local(g) == lg))
                                def _():
                                    pool(layer, last - j, lg)
                        each_group(distance, act)

                @pl.when(more & (rep == reps - 1))
                def _():
                    arrive(turn + 1)

    rescale(layers - 1, 0)
    take_halo(layers - 1)
    for i in (1, 0):
        for lg in range(own_groups):
            normalise_part(lg, i)
            pool(layers - 1, i, lg)

        @pl.loop(0, 2 - i)
        def _(j):
            finish(layers - 1, 1 + i - j)

    for way in range(2):
        for turn in range(turns):
            ring_copy(layers - 1, 1, way, turn, 0).wait_send()


def body(sp, tp, stream, doc_ids, norm_gain, proj_in, mix_pool, pool_gain, proj_out):
    layers, model_dev, chan_dev = proj_in.shape
    tokens = stream.shape[0]
    rows = tokens // CHUNKS
    channels = chan_dev * sp
    half = channels // 2
    group = mix_pool.shape[-1]
    own = half // group
    dma, vmem = pltpu.SemaphoreType.DMA, pltpu.VMEM
    local, remote = pl.BlockSpec(memory_space=pltpu.VMEM), pl.BlockSpec(memory_space=pl.ANY)
    return pl.pallas_call(
        functools.partial(mixer, sp, tp),
        out_shape=pltpu.VMEM(stream.shape, BF16),
        in_specs=[remote, local, local, remote, local, local, remote],
        out_specs=local,
        scratch_shapes=[
            vmem((layers, model_dev, channels), BF16),
            vmem((layers, channels, model_dev), BF16),
            vmem((tokens, model_dev), BF16),
            vmem((own, CHUNKS, rows, group), BF16),
            vmem((own, CHUNKS, rows, group), BF16),
            vmem((own, CHUNKS, rows, group), BF16),
            vmem((own, CHUNKS, rows, group), BF16),
            vmem((2, own, CHUNKS, rows, group), BF16),
            vmem((CHUNKS, rows, channels), BF16),
            vmem((own, HALO + tokens, group), BF16),
            vmem((layers, own, HALO, group), BF16),
            vmem((CHUNKS, 1, rows), F32),
            vmem((2, CHUNKS, 3, 1, rows), F32),
            vmem((CHUNKS, rows, 128), F32),
            vmem((2 * HALO + tokens, 128), F32),
            vmem((2 * HALO, 128), F32),
            vmem((HALO + tokens, 128), F32),
            vmem((4, tokens, 128), F32),
            vmem((layers, 1, model_dev), F32),
            vmem((layers, 1, half), F32),
            dma((CHUNKS,)), dma((layers, 2)),
            dma, dma,
            dma((2, sp - 1)), dma((2, sp - 1)),
            dma((CHUNKS,)), dma((2, CHUNKS)),
            dma((CHUNKS,)), dma((own, CHUNKS)),
            dma((CHUNKS,)), dma((2, own, CHUNKS)), dma((own,)),
            dma((CHUNKS,)), dma((CHUNKS,)),
            dma((layers,)), dma((layers,)),
        ],
        compiler_params=pltpu.CompilerParams(
            collective_id=0, has_side_effects=True, vmem_limit_bytes=56 * 2**20),
    )(stream, doc_ids.reshape(-1, 128), norm_gain, proj_in, mix_pool, pool_gain, proj_out)


span_reach = 15


def shifted(value, axis, steps):
    count = lax.axis_size(axis)
    initial, last = (max(0, -steps), min(count, count - steps))
    return lax.ppermute(value, axis, [(source, source + steps) for source in range(initial, last)])


def span_pool(padded, labels, widths):
    kept = padded.shape[0] - span_reach
    own_label = labels[span_reach:]
    summed = jnp.zeros((kept, padded.shape[1]), jnp.float32)
    counted = jnp.zeros((kept, padded.shape[1]), jnp.float32)
    for offset in range(span_reach + 1):
        first = span_reach - offset
        member = (labels[first : first + kept] == own_label)[:, None] & (offset < widths)[None, :]
        factor = member.astype(jnp.float32)
        summed = summed + padded[first : first + kept] * factor
        counted = counted + factor
    return summed / counted - padded[span_reach:]


def plain_body(stream, doc_ids, norm_gain, proj_in, mix_pool, pool_gain, proj_out):
    width_dev = stream.shape[1]
    tp_count = lax.axis_size("tp")
    model_width = width_dev * tp_count
    group_size = mix_pool.shape[2]
    channels = proj_in.shape[2] * lax.axis_size("sp")
    local = channels // tp_count
    groups_dev = local // group_size
    column = lax.axis_index("tp")
    chan_ids = column * local + jnp.arange(local, dtype=jnp.int32)
    widths = jnp.left_shift(jnp.int32(2), chan_ids // group_size % 4)
    labels = (doc_ids + 1).astype(jnp.bfloat16)
    hidden_state = stream
    layer_count = proj_in.shape[0]
    in_whole, out_whole = (
        lax.all_gather(proj_in, "sp", axis=2, tiled=True),
        lax.all_gather(proj_out, "sp", axis=1, tiled=True),
    )
    for layer in range(layer_count):
        row_count = hidden_state.shape[0]
        wide = hidden_state.astype(jnp.float32)
        own_squares = jnp.sum(wide * wide, axis=1)
        gain = lax.dynamic_slice_in_dim(norm_gain[layer], column * width_dev, width_dev).astype(
            jnp.float32
        )
        gained = (wide * gain[None, :]).astype(jnp.bfloat16)
        partial_value = jnp.dot(gained, in_whole[layer], preferred_element_type=jnp.float32)
        squares = lax.psum(own_squares, "tp")
        summed_in = lax.psum_scatter(
            partial_value.astype(jnp.bfloat16), "tp", scatter_dimension=1, tiled=True
        ).astype(jnp.float32)
        row_scale = lax.rsqrt(squares / model_width + EPSILON)
        mixed_in = (summed_in * row_scale[:, None]).astype(jnp.bfloat16)
        before, before_labels = shifted((mixed_in[-span_reach:], labels[-span_reach:]), "sp", 1)
        padded = jnp.concatenate([before, mixed_in], axis=0).astype(jnp.float32)
        tags = jnp.concatenate([before_labels, labels], axis=0)
        pooled = span_pool(padded, tags, widths).astype(jnp.bfloat16)
        grouped = pooled.reshape(row_count, groups_dev, group_size)
        mixing = lax.dynamic_slice_in_dim(mix_pool[layer], column * groups_dev, groups_dev, 0)
        blended = jnp.einsum(
            "tgc,gcd->tgd", grouped, mixing, preferred_element_type=jnp.float32
        ).reshape(row_count, local)
        scale = lax.dynamic_slice_in_dim(pool_gain[layer], column * local, local).astype(
            jnp.float32
        )
        mixed = (blended * scale[None, :]).astype(jnp.bfloat16)
        full_mixed = lax.all_gather(mixed, "tp", axis=1, tiled=True)
        update = jnp.dot(full_mixed, out_whole[layer], preferred_element_type=jnp.float32)
        hidden_state = (wide + update).astype(jnp.bfloat16)
    return hidden_state


def solution(mesh):
    sp, tp = mesh.shape["sp"], mesh.shape["tp"]
    in_specs = (P("sp", "tp"), P("sp"), P(), P(None, "tp", "sp"), P(), P(), P(None, "sp", "tp"))

    def whole(stream, doc_ids, norm_gain, proj_in, mix_pool, pool_gain, proj_out):
        layers, _, channels = proj_in.shape
        group = mix_pool.shape[2]
        fits = (tp == 4 and sp == RING and layers == LAYERS and channels == sp * group and group == 128
                and mix_pool.shape[1] % 8 == 0 and stream.shape[0] % (sp * CHUNKS * 128) == 0)
        part = functools.partial(body, sp, tp) if fits else plain_body
        return jax.shard_map(part, mesh=mesh, in_specs=in_specs, out_specs=P("sp", "tp"), check_vma=False)(
            stream, doc_ids, norm_gain, proj_in, mix_pool, pool_gain, proj_out)

    return whole
```
